128 devices in a mesh: sp: 16 (over z, x), tp: 8 (over y, core).
Axes of the slice: x: 4, y: 4, z: 4, core: 2. Of those that a mesh axis runs over, the one named last changes fastest.
Arguments:
- tokens: bfloat16 [8192, 4096], P('sp'), may hold values from -6 to 6
- norm_gain: float32 [4096], replicated, may hold values from 0.1 to 1.9
- w_pool_in: bfloat16 [4096, 2048], P(None, 'tp'), may hold values from -0.09375 to 0.09375
- w_query: bfloat16 [4096, 2048], P(None, 'tp'), may hold values from -0.15625 to 0.15625
- w_key: bfloat16 [4096, 2048], P(None, 'tp'), may hold values from -0.15625 to 0.15625
- w_value: bfloat16 [4096, 2048], P(None, 'tp'), may hold values from -0.09375 to 0.09375
- pool_mix: bfloat16 [32, 64, 64], P('tp'), may hold values from -0.75 to 0.75
- pool_scale: float32 [2048], P('tp'), may hold values from 0.1 to 1.9
- lam: float32 [16], P('tp'), may hold values from 0.3 to 0.8
- head_gain: float32 [128], replicated, may hold values from 0.1 to 1.9
- pool_proj: bfloat16 [2048, 4096], P('tp'), may hold values from -0.125 to 0.125
- attn_proj: bfloat16 [2048, 4096], P('tp'), may hold values from -0.125 to 0.125
Outputs:
- mixed: bfloat16 [8192, 4096], P(('sp', 'tp'))
The draws below stay inside these ranges and needn't reach their ends.
All inputs are finite; a program needn't handle non-finite values.
Results may differ from the reference program's by a relative error of at most 0.015.
Values may be sent and summed in bfloat16 or wider, within the bound.
A program may use at most 128 MiB of HBM per device.

```python
import jax
import jax.numpy as jnp
from jax import lax

D = 4096
GROUPS = 32
GDIM = 64
HEADS = 16
HEAD = 64
VDIM = 128
SEGMENT = 64
REACH = 16
POOL = 2048
TOKENS = 8192
N_TP = 8


def weight_noise(key, stream_id):
    drawn = 1.3 * jax.random.normal(jax.random.fold_in(key, stream_id), (D, HEADS * 2 * HEAD), jnp.float32)
    return jnp.clip(drawn, -7.8, 7.8) * D ** (-0.5)


def draw_tokens(key, part):
    noise_key = jax.random.fold_in(key, 11)
    drawn = jax.random.normal(noise_key, (TOKENS, D), jnp.float32)
    return jnp.clip(drawn, -6.0, 6.0).astype(jnp.bfloat16)


def draw_w_query(key, part):
    noise_part = weight_noise(key, 21)
    drawn = noise_part
    return drawn.astype(jnp.bfloat16)


def draw_w_key(key, part):
    noise_part = weight_noise(key, 22)
    drawn = noise_part
    return drawn.astype(jnp.bfloat16)


def shard_levels(rng, shape, split, smallest, largest):
    level = 1.0
    for axis_at, shards_of in split:
        heights = jax.random.uniform(jax.random.fold_in(jax.random.fold_in(rng, 6), axis_at), (shards_of,), jnp.float32, smallest / len(split), largest / len(split))
        level = level * jnp.repeat(jnp.exp(heights), shape[axis_at] // shards_of).reshape((-1,) + (1,) * (len(shape) - 1 - axis_at))
    return level


def scatter_about(rng, extent, deviation, most, pieces=(), kind=jnp.bfloat16):
    factor_of = shard_levels(rng, extent, pieces, -0.22, 0.18) if pieces else 1.0
    values = jax.random.normal(rng, extent, jnp.float32) * deviation * factor_of
    return jnp.minimum(jnp.maximum(values, -most), most).astype(kind)


def setup_inputs(seed: int = 0) -> dict:
    splits = jax.random.split(jax.random.key(seed), 13)
    tokens = draw_tokens(jax.random.fold_in(splits[12], 71), 0)
    norm_gain = jnp.clip(1.0 + 0.18 * jax.random.normal(splits[1], (D,), jnp.float32), 0.1, 1.9)
    w_pool_in = scatter_about(splits[2], (D, POOL), D ** -0.5, 0.09375, ((1, 8),))
    w_query = draw_w_query(jax.random.fold_in(splits[12], 71), 0)
    w_key = draw_w_key(jax.random.fold_in(splits[12], 71), 0)
    w_value = scatter_about(splits[5], (D, HEADS * VDIM), D ** -0.5, 0.09375, ((1, 8),))
    pool_mix = scatter_about(splits[6], (GROUPS, GDIM, GDIM), GDIM ** -0.5, 0.75, ((0, 8),))
    pool_scale = jnp.clip(1.0 + 0.18 * jax.random.normal(splits[7], (POOL,), jnp.float32), 0.1, 1.9)
    lam = jnp.clip(0.3 + 0.5 * jax.random.uniform(splits[8], (HEADS,), jnp.float32) ** shard_levels(splits[8], (HEADS,), ((0, 8),), -0.2, 0.2), 0.3, 0.8)
    head_gain = jnp.clip(1.0 + 0.18 * jax.random.normal(splits[9], (VDIM,), jnp.float32), 0.1, 1.9)
    pool_proj = scatter_about(splits[10], (POOL, D), POOL ** -0.5, 0.125, ((0, 8),))
    attn_proj = scatter_about(splits[11], (HEADS * VDIM, D), (HEADS * VDIM) ** -0.5, 0.125, ((0, 8),))
    return {"tokens": tokens, "norm_gain": norm_gain, "w_pool_in": w_pool_in, "w_query": w_query, "w_key": w_key, "w_value": w_value, "pool_mix": pool_mix, "pool_scale": pool_scale, "lam": lam, "head_gain": head_gain, "pool_proj": pool_proj, "attn_proj": attn_proj}


eps_norm = 1e-06
neg_big = -1e+30
out_scale = 0.8

def reference(tokens, norm_gain, w_pool_in, w_query, w_key, w_value, pool_mix, pool_scale, lam, head_gain, pool_proj, attn_proj):
    wide = tokens.astype(jnp.float32)
    normed = (wide * lax.rsqrt(lax.optimization_barrier(jnp.mean(wide * wide, axis=-1, keepdims=True)) + eps_norm) * norm_gain).astype(jnp.bfloat16)
    pool_in = jnp.dot(normed, w_pool_in, preferred_element_type=jnp.float32).astype(jnp.bfloat16)
    query = jnp.dot(normed, w_query, preferred_element_type=jnp.float32).astype(jnp.bfloat16)
    keys = jnp.dot(normed, w_key, preferred_element_type=jnp.float32).astype(jnp.bfloat16)
    values = jnp.dot(normed, w_value, preferred_element_type=jnp.float32).astype(jnp.bfloat16)
    padded = jnp.concatenate([jnp.zeros((REACH - 1, POOL), jnp.float32), pool_in.astype(jnp.float32)], 0)
    channel_group = jnp.arange(POOL, dtype=jnp.int32) // GDIM
    window = 2 ** (1 + channel_group % 4)
    total = jnp.zeros((TOKENS, POOL), jnp.float32)
    for back in range(REACH):
        low = REACH - 1 - back
        total = total + jnp.where(back < window[None, :], padded[low:low + TOKENS], 0.0)
    position = jnp.arange(TOKENS, dtype=jnp.int32)
    count = jnp.minimum(position[:, None] + 1, window[None, :]).astype(jnp.float32)
    pooled = (total / count - pool_in.astype(jnp.float32)).astype(jnp.bfloat16)
    grouped = jnp.einsum('sgi,gio->sgo', pooled.reshape(TOKENS, GROUPS, GDIM).astype(jnp.float32), pool_mix.astype(jnp.float32))
    pool_out = (grouped.reshape(TOKENS, POOL) * pool_scale).astype(jnp.bfloat16)
    query_heads = query.reshape(TOKENS, HEADS, 2, HEAD).transpose(1, 0, 2, 3)
    key_heads = keys.reshape(TOKENS, HEADS, 2, HEAD).transpose(1, 0, 2, 3)
    value_heads = values.reshape(TOKENS, HEADS, VDIM).transpose(1, 0, 2)
    segments = position // SEGMENT
    block = min(TOKENS, 512) if TOKENS % min(TOKENS, 512) == 0 else TOKENS
    scale = HEAD ** (-0.5)

    def one_head(args):
        query_head, key_head, value_head, lam_head = args

        def one_block(index):
            first = (index * block).astype(jnp.int32)
            query_block = lax.dynamic_slice_in_dim(query_head, first, block, 0)
            query_seg = (first + jnp.arange(block, dtype=jnp.int32)) // SEGMENT
            allowed = segments[None, :] <= query_seg[:, None]
            results = []
            for which in range(2):
                scores = jnp.dot(query_block[:, which], key_head[:, which].T, preferred_element_type=jnp.float32) * scale
                masked = jnp.where(allowed, scores, neg_big)
                top = lax.optimization_barrier(jnp.max(masked, axis=-1, keepdims=True))
                probs = jnp.where(allowed, jnp.exp(masked - top), 0.0)
                weighted = jnp.dot(probs.astype(jnp.bfloat16), value_head, preferred_element_type=jnp.float32)
                results.append(weighted / lax.optimization_barrier(jnp.sum(probs, axis=-1, keepdims=True)))
            blend = results[0] - lam_head * results[1]
            scaled = blend * lax.rsqrt(lax.optimization_barrier(jnp.mean(blend * blend, axis=-1, keepdims=True)) + eps_norm) * head_gain * out_scale
            return scaled.astype(jnp.bfloat16)
        return lax.map(one_block, jnp.arange(TOKENS // block, dtype=jnp.int32))
    per_head = lax.map(one_head, (query_heads, key_heads, value_heads, lam))
    attn_out = per_head.reshape(HEADS, TOKENS, VDIM).transpose(1, 0, 2).reshape(TOKENS, HEADS * VDIM)
    pool_share = POOL // N_TP
    attn_share = HEADS * VDIM // N_TP
    summed = jnp.zeros((TOKENS, D), jnp.float32)
    for part in range(N_TP):
        term = jnp.dot(pool_out[:, part * pool_share:(part + 1) * pool_share], pool_proj[part * pool_share:(part + 1) * pool_share], preferred_element_type=jnp.float32)
        term = term + jnp.dot(attn_out[:, part * attn_share:(part + 1) * attn_share], attn_proj[part * attn_share:(part + 1) * attn_share], preferred_element_type=jnp.float32)
        summed = summed + lax.optimization_barrier(term.astype(jnp.bfloat16)).astype(jnp.float32)
    return summed.astype(jnp.bfloat16)
```

```python
import jax
import jax.numpy as jnp
from jax import lax
from jax.experimental import pallas as pl
from jax.experimental.pallas import tpu as pltpu
from jax.sharding import PartitionSpec as P

EPS = 1e-6
NEG = -1e30
LOG2E = 1.4426950408889634
ROWS = 512
WIDE = 4096
SEG = 64
BF = jnp.bfloat16
F32 = jnp.float32
MESH_ID = pl.DeviceIdType.MESH
ANY = pl.BlockSpec(memory_space=pl.ANY)
VM = pl.BlockSpec(memory_space=pltpu.VMEM)
SM = pl.BlockSpec(memory_space=pltpu.SMEM)


def project_kernel(tok, gain, w_k, w_v, w_q, w_p, lam, kv_out, q_out, pool_out, lam_out,
                   raw, normed, wts, tok_sem, w_sem):
    loads = []
    for r in range(4):
        cp = pltpu.make_async_copy(tok.at[pl.ds(r * 128, 128)], raw.at[pl.ds(r * 128, 128)], tok_sem.at[r])
        cp.start()
        loads.append(cp)
    w_loads = []
    for i, w in enumerate((w_k, w_v, w_q, w_p)):
        cp = pltpu.make_async_copy(w, wts.at[i], w_sem.at[i])
        cp.start()
        w_loads.append(cp)
    for hh in range(2):
        lam_out[hh] = jnp.full((8, 128), lam[hh], F32)

    for r in range(4):
        loads[r].wait()

        @pl.loop(0, 8)
        def _(i):
            rows = pl.ds(pl.multiple_of(r * 128 + i * 16, 16), 16)
            wide = raw[rows].astype(F32)
            scale = lax.rsqrt(jnp.mean(wide * wide, axis=-1, keepdims=True) + EPS)
            normed[rows] = (wide * scale * gain[...]).astype(BF)

    def product(i):
        w_loads[i].wait()
        return jnp.dot(normed[...], wts[i], preferred_element_type=F32)

    keys = product(0).astype(BF)
    for hh in range(2):
        for hf in range(2):
            kv_out[hh, hf, 0:256] = keys[256 * hf:256 * hf + 256, 128 * hh:128 * hh + 128]
    values = product(1)
    for hh in range(2):
        for hf in range(2):
            for j in range(2):
                first = 256 * hf + 128 * j
                tile = values[first:first + 128, 128 * hh:128 * hh + 128]
                kv_out[hh, hf, 256 + 128 * j:384 + 128 * j] = tile.T.astype(BF)
    query = product(2).astype(BF)
    for hh in range(2):
        q_out[hh] = query[:, 128 * hh:128 * hh + 128]
    pool_out[...] = product(3).astype(BF)


def mixer_kernel(kv_in, q_in, pool_in, lam_in, pool_mix, pool_scale, head_gain, pool_proj, attn_proj,
                 out,
                 kv, qraw, qcat, lamb, rim, acc, top, den, ao, ab, pooled, w_out, pbuf, dbuf, sbuf, relay, fin,
                 w_sem, a2a_send, kv_recv, q_send, q_recv, lam_send, lam_recv, rim_send, rim_recv,
                 zp_send, zm_send, dd_send, ret_send, ret_recv, pd_send, pd_recv, y_send, y_recv):
    sp = lax.axis_index("sp")
    tp = lax.axis_index("tp")
    z, x = lax.div(sp, 4), lax.rem(sp, 4)
    y, c = lax.div(tp, 2), lax.rem(tp, 2)

    def wrap(i):
        return lax.rem(i + 4, 4)

    def dev(zz, xx, cc):
        return (zz * 4 + xx, y * 2 + cc)

    me = (sp, tp)

    def is_me(d):
        return (d[0] == sp) & (d[1] == tp)

    core_src = lax.div(x, 2)
    odd_row = lax.rem(z, 2) == 1
    zq = jnp.where(odd_row, 3 - x, x)
    cq = jnp.where((z == 0) | (z == 3), 0, 1)
    sq = lax.div(z, 2)
    qb = [jnp.where(c == 0, z, 7 - z), jnp.where(c == 0, 15 - z, 8 + z)]
    partner = dev(z, x, 1 - c)
    z_up, z_dn = dev(wrap(z + 1), x, c), dev(wrap(z - 1), x, c)
    y_up = (sp, wrap(y + 1) * 2 + c)
    y_dn = (sp, wrap(y - 1) * 2 + c)
    nxt = (lax.rem(sp + 1, 16), tp)
    prv = (lax.rem(sp + 15, 16), tp)
    a2a_dst = [[dev(z, 2 * c + hh, hf) for hf in range(2)] for hh in range(2)]
    q_dst = [dev(zq, 2 * c + hh, cq) for hh in range(2)]
    q_src = [dev(lax.div(qb[s], 4), lax.rem(qb[s], 4), core_src) for s in range(2)]

    w_loads = [pltpu.make_async_copy(pool_proj, w_out.at[pl.ds(0, 256)], w_sem.at[0]),
               pltpu.make_async_copy(attn_proj, w_out.at[pl.ds(256, 256)], w_sem.at[1])]
    for cp in w_loads:
        cp.start()

    barrier = pltpu.get_barrier_semaphore()

    def greet(d):
        pl.semaphore_signal(barrier, inc=1, device_id=d, device_id_type=MESH_ID)

    greeted = [dev(z, xk, core_src) for xk in range(4)] + q_src + q_dst + [z_up, z_dn, partner, y_up, y_dn, prv]
    for d in greeted:
        greet(d)
    pl.semaphore_wait(barrier, len(greeted))

    def remote(src, dst, ssem, rsem, d):
        return pltpu.make_async_remote_copy(src_ref=src, dst_ref=dst, send_sem=ssem, recv_sem=rsem,
                                            device_id=d, device_id_type=MESH_ID)

    def send_any(src, dst, ssem, rsem, d):
        @pl.when(is_me(d))
        def _():
            pltpu.make_async_copy(src, dst, rsem).start()

        @pl.when(jnp.logical_not(is_me(d)))
        def _():
            remote(src, dst, ssem, rsem, d).start()

    def sent_any(src, dst, ssem, rsem, d):
        @pl.when(jnp.logical_not(is_me(d)))
        def _():
            remote(src, dst, ssem, rsem, d).wait_send()

    def arrived(dst, rsem):
        pltpu.make_async_copy(dst, dst, rsem).wait()

    rim_args = (pool_in.at[pl.ds(ROWS - 16, 16)], rim, rim_send, rim_recv, nxt)
    remote(*rim_args).start()
    a2a_args = []
    for hh in range(2):
        for hf in range(2):
            a2a_args.append((kv_in.at[hh, hf], kv.at[z, hf, x], a2a_send.at[hh, hf], kv_recv.at[0, hf, x],
                             a2a_dst[hh][hf]))
    q_args = []
    for hh in range(2):
        q_args.append((q_in.at[hh], qraw.at[sq], q_send.at[hh], q_recv.at[sq], q_dst[hh]))
        q_args.append((lam_in.at[hh], lamb.at[sq], lam_send.at[hh], lam_recv.at[sq], q_dst[hh]))
    for a in a2a_args + q_args:
        send_any(*a)

    arrived(rim, rim_recv)
    remote(*rim_args).wait_send()
    edge = jnp.where(sp == 0, 0.0, rim[...].astype(F32))
    own = pool_in[...].astype(F32)
    line = jnp.concatenate([edge, own], axis=0)
    s2 = line + pltpu.roll(line, 1, 0)
    s4 = s2 + pltpu.roll(s2, 2, 0)
    s8 = s4 + pltpu.roll(s4, 4, 0)
    s16 = s8 + pltpu.roll(s8, 8, 0)
    lane = lax.broadcasted_iota(jnp.int32, (1, 256), 1)
    total = jnp.where(lane < 64, s2, jnp.where(lane < 128, s4, jnp.where(lane < 192, s8, s16)))[16:]
    window = jnp.where(lane < 64, 2, jnp.where(lane < 128, 4, jnp.where(lane < 192, 8, 16)))
    position = sp * ROWS + lax.broadcasted_iota(jnp.int32, (ROWS, 256), 0)
    count = jnp.minimum(position + 1, window).astype(F32)
    mixed_in = (total / count - own).astype(BF)
    spread = (lax.rem(lax.broadcasted_iota(jnp.int32, (64, 256), 1), 64)
              == lax.broadcasted_iota(jnp.int32, (64, 256), 0)).astype(F32).astype(BF)
    wide_mix = jnp.dot(pool_mix[...], spread, preferred_element_type=F32)
    same = (lax.div(lax.broadcasted_iota(jnp.int32, (256, 256), 0), 64)
            == lax.div(lax.broadcasted_iota(jnp.int32, (256, 256), 1), 64))
    block_mix = jnp.where(same, wide_mix, 0.0).astype(BF)
    grouped = jnp.dot(mixed_in, block_mix, preferred_element_type=F32)
    pooled[...] = (grouped * pool_scale[...]).astype(BF)

    def dd_args(rel, xk):
        piece = kv.at[wrap(z + rel), c, xk]
        return (piece, piece, dd_send.at[rel, xk], kv_recv.at[rel, c, xk], partner)

    def up_args(rel, xk):
        piece = kv.at[wrap(z + rel), c, xk]
        return (piece, piece, zp_send.at[rel & 1, xk], kv_recv.at[(rel + 3) % 4, c, xk], z_up)

    def dn_args(rel, xk):
        piece = kv.at[wrap(z + rel), c, xk]
        return (piece, piece, zm_send.at[rel & 1, xk], kv_recv.at[(rel + 1) % 4, c, xk], z_dn)

    def mine(rel, xk):
        arrived(kv.at[wrap(z + rel), c, xk], kv_recv.at[rel, c, xk])

    for xk in range(4):
        mine(0, xk)
        remote(*up_args(0, xk)).start()
        if xk >= 2:
            remote(*dn_args(0, xk)).start()
        remote(*dd_args(0, xk)).start()
    for xk in range(2):
        remote(*dn_args(0, xk)).start()

    for s in range(2):
        arrived(qraw.at[s], q_recv.at[s])
        arrived(lamb.at[s], lam_recv.at[s])
        q = qraw[s] * jnp.asarray(0.125, BF)
        first = lax.broadcasted_iota(jnp.int32, (ROWS, 128), 1) < 64
        qcat[s, 0] = jnp.where(first, q, jnp.zeros_like(q))
        qcat[s, 1] = jnp.where(first, jnp.zeros_like(q), q)
        for m in range(2):
            top[s, m] = jnp.full((1, ROWS), NEG, F32)
            den[s, m] = jnp.zeros((1, ROWS), F32)
            acc[s, m] = jnp.zeros((128, ROWS), F32)

    def attend(s, zk, xk, masked):
        halves = [kv[zk, hf, xk] for hf in range(2)]
        keys = jnp.concatenate([h[:256] for h in halves], axis=0)
        vals = jnp.concatenate([h[256 + 128 * j:384 + 128 * j] for h in halves for j in range(2)], axis=1)
        for m in range(2):
            scores = lax.dot_general(keys, qcat[s, m], (((1,), (1,)), ((), ())),
                                     preferred_element_type=F32) * LOG2E
            if masked:
                allowed = (lax.div(lax.broadcasted_iota(jnp.int32, (ROWS, ROWS), 0), SEG)
                           <= lax.div(lax.broadcasted_iota(jnp.int32, (ROWS, ROWS), 1), SEG))
                scores = jnp.where(allowed, scores, NEG)
            old = top[s, m]
            new = jnp.maximum(old, jnp.max(scores, axis=0, keepdims=True))
            probs = jnp.exp2(scores - new)
            shrink = jnp.exp2(old - new)
            top[s, m] = new
            den[s, m] = den[s, m] * shrink + jnp.sum(probs, axis=0, keepdims=True)
            acc[s, m] = acc[s, m] * shrink + jnp.dot(vals, probs.astype(BF), preferred_element_type=F32)

    def visit(rel, xk):
        zk = wrap(z + rel)
        arrived(kv.at[zk, 1 - c, xk], kv_recv.at[rel, 1 - c, xk])
        block = zk * 4 + xk

        @pl.loop(0, 2)
        def _(s):
            target = jnp.where(s == 0, qb[0], qb[1])

            @pl.when(block < target)
            def _():
                attend(s, zk, xk, False)

            @pl.when(block == target)
            def _():
                attend(s, zk, xk, True)

    @pl.loop(0, 4)
    def _(xk):
        visit(0, xk)

    @pl.loop(0, 5)
    def _(i):
        @pl.when(i < 4)
        def _():
            mine(3, i)
            remote(*dd_args(3, i)).start()

            @pl.when(i < 2)
            def _():
                remote(*up_args(3, i)).start()

            j = lax.rem(i + 2, 4)
            mine(1, j)
            remote(*dd_args(1, j)).start()

            @pl.when(i < 2)
            def _():
                remote(*dn_args(1, j)).start()

        @pl.when(i > 0)
        def _():
            @pl.loop(0, 2)
            def _(side):
                k = jnp.where(side == 0, i - 1, lax.rem(i + 1, 4))
                visit(jnp.where(side == 0, 3, 1), k)

    def turn(i):
        return jnp.where(i == 0, 0, jnp.where(i == 1, 2, jnp.where(i == 2, 1, 3)))

    @pl.loop(0, 5)
    def _(i):
        @pl.when(i < 4)
        def _():
            k = turn(i)
            mine(2, k)
            remote(*dd_args(2, k)).start()

        @pl.when(i > 0)
        def _():
            visit(2, turn(i - 1))

    ret_args = []
    for s in range(2):
        o1 = acc[s, 0] / den[s, 0]
        o2 = acc[s, 1] / den[s, 1]
        blend = o1 - lamb[s][0:1, 0:1] * o2
        scaled = blend * lax.rsqrt(jnp.mean(blend * blend, axis=0, keepdims=True) + EPS)
        ao[s] = (scaled.T * head_gain[...] * 0.8).astype(BF)
        mine_h = lax.rem(x, 2)
        a = (ao.at[s], ab.at[mine_h], ret_send.at[s], ret_recv.at[mine_h], q_src[s])
        send_any(*a)
        ret_args.append(a)

    for a in a2a_args + q_args:
        sent_any(*a)
    for xk in range(4):
        remote(*up_args(0, xk)).wait_send()
        remote(*dn_args(0, xk)).wait_send()
        for rel in range(4):
            remote(*dd_args(rel, xk)).wait_send()
    for xk in range(2):
        remote(*up_args(3, xk)).wait_send()
        remote(*dn_args(1, xk + 2)).wait_send()

    for cp in w_loads:
        cp.wait()
    for hh in range(2):
        arrived(ab.at[hh], ret_recv.at[hh])

    order = [wrap(y + 2), wrap(y + 1), wrap(y - 1), y]

    def pd_args(h, k):
        return (pbuf.at[h, 2 * order[k] + 1 - c], dbuf.at[h, k], pd_send.at[h, k], pd_recv.at[h, k], partner)

    for h in range(2):
        @pl.loop(0, 4)
        def _(n):
            cols = pl.ds(pl.multiple_of(h * 2048 + n * 512, 512), 512)
            to = pl.ds(pl.multiple_of(n * 512, 512), 512)
            feats = jnp.concatenate([pooled[...], ab[0], ab[1]], axis=1)
            term = jnp.dot(feats, w_out[:, cols], preferred_element_type=F32)
            pbuf[h, :, :, to] = term.astype(BF).reshape(8, 64, 512)

        for k in range(4):
            remote(*pd_args(h, k)).start()

    def chip_sum(h, k):
        arrived(dbuf.at[h, k], pd_recv.at[h, k])
        return pbuf[h, 2 * order[k] + c].astype(F32) + dbuf[h, k].astype(F32)

    A, B = 0, 1
    y_args = [
        (sbuf.at[0], relay.at[0], y_send.at[0], y_recv.at[0], y_up),
        (sbuf.at[1], relay.at[1], y_send.at[1], y_recv.at[1], y_dn),
        (sbuf.at[2], fin.at[0, B], y_send.at[2], y_recv.at[2], y_up),
        (sbuf.at[3], fin.at[1, A], y_send.at[3], y_recv.at[3], y_dn),
        (sbuf.at[4], fin.at[0, A], y_send.at[4], y_recv.at[4], y_up),
        (sbuf.at[5], fin.at[1, B], y_send.at[5], y_recv.at[5], y_dn),
    ]

    def y_go(i, value):
        sbuf[i] = value.astype(BF)
        remote(*y_args[i]).start()

    y_go(0, chip_sum(A, 0))
    y_go(1, chip_sum(B, 0))
    y_go(3, chip_sum(A, 2))
    y_go(2, chip_sum(B, 1))
    up = chip_sum(A, 1)
    arrived(relay.at[0], y_recv.at[0])
    y_go(4, up + relay[0].astype(F32))
    dn = chip_sum(B, 2)
    arrived(relay.at[1], y_recv.at[1])
    y_go(5, dn + relay[1].astype(F32))

    arrived(fin.at[0, B], y_recv.at[2])
    arrived(fin.at[1, A], y_recv.at[3])
    arrived(fin.at[0, A], y_recv.at[4])
    arrived(fin.at[1, B], y_recv.at[5])
    for h in range(2):
        whole = chip_sum(h, 3) + fin[0, h].astype(F32) + fin[1, h].astype(F32)
        out[:, 2048 * h:2048 * h + 2048] = whole.astype(BF)

    for a in ret_args:
        sent_any(*a)
    for h in range(2):
        for k in range(4):
            remote(*pd_args(h, k)).wait_send()
    for a in y_args:
        remote(*a).wait_send()


def body(tokens, norm_gain, w_pool_in, w_query, w_key, w_value, pool_mix, pool_scale, lam, head_gain,
         pool_proj, attn_proj):
    sd = jax.ShapeDtypeStruct
    kv, q, pool_in, lam_tile = pl.pallas_call(
        project_kernel,
        out_shape=(sd((2, 2, 512, 128), BF), sd((2, ROWS, 128), BF), sd((ROWS, 256), BF), sd((2, 8, 128), F32)),
        in_specs=[ANY, VM, ANY, ANY, ANY, ANY, SM],
        out_specs=(VM, VM, VM, VM),
        scratch_shapes=[
            pltpu.VMEM((ROWS, WIDE), BF), pltpu.VMEM((ROWS, WIDE), BF), pltpu.VMEM((4, WIDE, 256), BF),
            pltpu.SemaphoreType.DMA((4,)), pltpu.SemaphoreType.DMA((4,)),
        ],
        compiler_params=pltpu.CompilerParams(vmem_limit_bytes=40 << 20),
        name="project",
    )(tokens, norm_gain.reshape(1, WIDE), w_key, w_value, w_query, w_pool_in, lam)

    dma = pltpu.SemaphoreType.DMA
    return pl.pallas_call(
        mixer_kernel,
        out_shape=sd((64, WIDE), BF),
        in_specs=[VM, VM, VM, VM, VM, VM, VM, ANY, ANY],
        out_specs=VM,
        scratch_shapes=[
            pltpu.VMEM((4, 2, 4, 512, 128), BF),
            pltpu.VMEM((2, ROWS, 128), BF),
            pltpu.VMEM((2, 2, ROWS, 128), BF),
            pltpu.VMEM((2, 8, 128), F32),
            pltpu.VMEM((16, 256), BF),
            pltpu.VMEM((2, 2, 128, ROWS), F32),
            pltpu.VMEM((2, 2, 1, ROWS), F32),
            pltpu.VMEM((2, 2, 1, ROWS), F32),
            pltpu.VMEM((2, ROWS, 128), BF),
            pltpu.VMEM((2, ROWS, 128), BF),
            pltpu.VMEM((ROWS, 256), BF),
            pltpu.VMEM((512, WIDE), BF),
            pltpu.VMEM((2, 8, 64, 2048), BF),
            pltpu.VMEM((2, 4, 64, 2048), BF),
            pltpu.VMEM((6, 64, 2048), BF),
            pltpu.VMEM((2, 64, 2048), BF),
            pltpu.VMEM((2, 2, 64, 2048), BF),
            dma((2,)), dma((2, 2)), dma((4, 2, 4)), dma((2,)), dma((2,)), dma((2,)), dma((2,)),
            dma, dma, dma((2, 4)), dma((2, 4)), dma((4, 4)), dma((2,)), dma((2,)),
            dma((2, 4)), dma((2, 4)), dma((6,)), dma((6,)),
        ],
        compiler_params=pltpu.CompilerParams(vmem_limit_bytes=60 << 20, collective_id=0, has_side_effects=True),
        name="mixer",
    )(kv, q, pool_in, lam_tile, pool_mix.reshape(256, 64), pool_scale.reshape(1, 256), head_gain.reshape(1, 128),
      pool_proj, attn_proj)


def solution(mesh):
    return jax.shard_map(
        body,
        mesh=mesh,
        in_specs=(P("sp", None), P(), P(None, "tp"), P(None, "tp"), P(None, "tp"), P(None, "tp"),
                  P("tp", None, None), P("tp"), P("tp"), P(), P("tp", None), P("tp", None)),
        out_specs=P(("sp", "tp"), None),
        check_vma=False,
    )
```

```python
import jax
import jax.numpy as jnp
from jax import lax
from jax.experimental import pallas as pl
from jax.experimental.pallas import tpu as pltpu
from jax.sharding import PartitionSpec as P

EPS = 1e-6
NEG = -1e30
LOG2E = 1.4426950408889634
ROWS = 512
WIDE = 4096
SEG = 64
BF = jnp.bfloat16
F32 = jnp.float32
MESH_ID = pl.DeviceIdType.MESH
ANY = pl.BlockSpec(memory_space=pl.ANY)
VM = pl.BlockSpec(memory_space=pltpu.VMEM)
SM = pl.BlockSpec(memory_space=pltpu.SMEM)


def mixer_kernel(tok, gain, w_k, w_v, w_q, w_p, lam, pool_mix, pool_scale, head_gain, pool_proj, attn_proj,
                 out,
                 raw, normed, wts, kv_in, q_in, pool_in, lam_in, kv, qraw, qcat, lamb, rim, acc, top, den, sbank_a, sbank_b, ao, ab, pooled, w_out, pbuf, dbuf, sbuf, relay, fin,
                 tok_sem, w_sem, a2a_send, kv_recv, q_send, q_recv, lam_send, lam_recv, rim_send, rim_recv,
                 zp_send, zm_send, dd_send, ret_send, ret_recv, pd_send, pd_recv, y_send, y_recv):
    sbank = (sbank_a, sbank_b)
    sp = lax.axis_index("sp")
    tp = lax.axis_index("tp")
    z, x = lax.div(sp, 4), lax.rem(sp, 4)
    y, c = lax.div(tp, 2), lax.rem(tp, 2)

    def wrap(i):
        return lax.rem(i + 4, 4)

    def dev(zz, xx, cc):
        return (zz * 4 + xx, y * 2 + cc)

    me = (sp, tp)

    def is_me(d):
        return (d[0] == sp) & (d[1] == tp)

    core_src = lax.div(x, 2)
    odd_row = lax.rem(z, 2) == 1
    zq = jnp.where(odd_row, 3 - x, x)
    cq = jnp.where((z == 0) | (z == 3), 0, 1)
    sq = lax.div(z, 2)
    qb = [jnp.where(c == 0, z, 7 - z), jnp.where(c == 0, 15 - z, 8 + z)]
    partner = dev(z, x, 1 - c)
    z_up, z_dn = dev(wrap(z + 1), x, c), dev(wrap(z - 1), x, c)
    y_up = (sp, wrap(y + 1) * 2 + c)
    y_dn = (sp, wrap(y - 1) * 2 + c)
    nxt = (lax.rem(sp + 1, 16), tp)
    prv = (lax.rem(sp + 15, 16), tp)
    a2a_dst = [[dev(z, 2 * c + hh, hf) for hf in range(2)] for hh in range(2)]
    q_dst = [dev(zq, 2 * c + hh, cq) for hh in range(2)]
    q_src = [dev(lax.div(qb[s], 4), lax.rem(qb[s], 4), core_src) for s in range(2)]

    def load(src, dst, sem):
        cp = pltpu.make_async_copy(src, dst, sem)
        cp.start()
        return cp

    tok_loads = [load(tok.at[pl.ds(r * 128, 128)], raw.at[pl.ds(r * 128, 128)], tok_sem.at[r]) for r in range(4)]
    in_loads = [load(w, wts.at[i], w_sem.at[i]) for i, w in enumerate((w_k, w_v, w_q, w_p))]
    w_loads = [load(pool_proj, w_out.at[pl.ds(0, 256)], w_sem.at[4]),
               load(attn_proj, w_out.at[pl.ds(256, 256)], w_sem.at[5])]

    barrier = pltpu.get_barrier_semaphore()

    def greet(d):
        pl.semaphore_signal(barrier, inc=1, device_id=d, device_id_type=MESH_ID)

    greeted = [dev(z, xk, core_src) for xk in range(4)] + q_src + q_dst + [z_up, z_dn, partner, y_up, y_dn, prv]
    for d in greeted:
        greet(d)

    def remote(src, dst, ssem, rsem, d):
        return pltpu.make_async_remote_copy(src_ref=src, dst_ref=dst, send_sem=ssem, recv_sem=rsem,
                                            device_id=d, device_id_type=MESH_ID)

    def send_any(src, dst, ssem, rsem, d):
        @pl.when(is_me(d))
        def _():
            pltpu.make_async_copy(src, dst, rsem).start()

        @pl.when(jnp.logical_not(is_me(d)))
        def _():
            remote(src, dst, ssem, rsem, d).start()

    def sent_any(src, dst, ssem, rsem, d):
        @pl.when(jnp.logical_not(is_me(d)))
        def _():
            remote(src, dst, ssem, rsem, d).wait_send()

    def arrived(dst, rsem):
        pltpu.make_async_copy(dst, dst, rsem).wait()

    for hh in range(2):
        lam_in[hh] = jnp.full((8, 128), lam[hh], F32)
    with jax.named_scope("norm"):
        for r in range(4):
            tok_loads[r].wait()

            @pl.loop(0, 8, unroll=4)
            def _(i):
                rows = pl.ds(pl.multiple_of(r * 128 + i * 16, 16), 16)
                wide = raw[rows].astype(F32)
                scale = lax.rsqrt(jnp.mean(wide * wide, axis=-1, keepdims=True) + EPS)
                normed[rows] = (wide * scale * gain[...]).astype(BF)

    def product(i):
        return jnp.dot(normed[...], wts[i], preferred_element_type=F32)

    with jax.named_scope("keys_values"):
        in_loads[0].wait()
        in_loads[1].wait()
        keys = product(0).astype(BF)
        values = product(1)
        for hh in range(2):
            for hf in range(2):
                kv_in[hh, hf, 0:256] = keys[256 * hf:256 * hf + 256, 128 * hh:128 * hh + 128]
                for j in range(2):
                    first = 256 * hf + 128 * j
                    tile = values[first:first + 128, 128 * hh:128 * hh + 128]
                    kv_in[hh, hf, 256 + 128 * j:384 + 128 * j] = tile.T.astype(BF)

    pl.semaphore_wait(barrier, len(greeted))

    a2a_args = []
    for hh in range(2):
        for hf in range(2):
            a2a_args.append((kv_in.at[hh, hf], kv.at[z, hf, x], a2a_send.at[hh, hf], kv_recv.at[0, hf, x],
                             a2a_dst[hh][hf]))
    for a in a2a_args:
        send_any(*a)

    def dd_args(rel, xk):
        piece = kv.at[wrap(z + rel), c, xk]
        return (piece, piece, dd_send.at[rel, xk], kv_recv.at[rel, c, xk], partner)

    def up_args(rel, xk):
        piece = kv.at[wrap(z + rel), c, xk]
        return (piece, piece, zp_send.at[rel & 1, xk], kv_recv.at[(rel + 3) % 4, c, xk], z_up)

    def dn_args(rel, xk):
        piece = kv.at[wrap(z + rel), c, xk]
        return (piece, piece, zm_send.at[rel & 1, xk], kv_recv.at[(rel + 1) % 4, c, xk], z_dn)

    def mine(rel, xk):
        arrived(kv.at[wrap(z + rel), c, xk], kv_recv.at[rel, c, xk])

    def at(off):
        return lax.rem(x + off, 4)

    def go(args):
        remote(*args).start()

    mine(0, at(0))
    go(up_args(0, at(0)))
    go(dn_args(0, at(0)))
    go(dd_args(0, at(0)))

    with jax.named_scope("query_pool"):
        in_loads[2].wait()
        in_loads[3].wait()
        query = product(2) * (0.125 * LOG2E)
        pool_in[...] = product(3).astype(BF)
        for hh in range(2):
            q_in[hh] = query[:, 128 * hh:128 * hh + 128].T.astype(BF)
    rim_args = (pool_in.at[pl.ds(ROWS - 16, 16)], rim, rim_send, rim_recv, nxt)
    go(rim_args)
    q_args = []
    for hh in range(2):
        q_args.append((q_in.at[hh], qraw.at[sq], q_send.at[hh], q_recv.at[sq], q_dst[hh]))
        q_args.append((lam_in.at[hh], lamb.at[sq], lam_send.at[hh], lam_recv.at[sq], q_dst[hh]))
    for a in q_args:
        send_any(*a)

    with jax.named_scope("own_near"):
        mine(0, at(1))
        go(up_args(0, at(1)))
        go(dd_args(0, at(1)))
        mine(0, at(3))
        go(dn_args(0, at(3)))
        go(up_args(0, at(3)))
        go(dd_args(0, at(3)))

    with jax.named_scope("pooling"):
        arrived(rim, rim_recv)
        edge = jnp.where(sp == 0, 0.0, rim[...].astype(F32))
        own = pool_in[...].astype(F32)
        lane = lax.broadcasted_iota(jnp.int32, (1, 128), 1)
        totals = []
        for side in range(2):
            cols = slice(128 * side, 128 * side + 128)
            line = jnp.concatenate([edge[:, cols], own[:, cols]], axis=0)
            s2 = line + pltpu.roll(line, 1, 0)
            s4 = s2 + pltpu.roll(s2, 2, 0)
            if side == 0:
                totals.append(jnp.where(lane < 64, s2, s4)[16:])
            else:
                s8 = s4 + pltpu.roll(s4, 4, 0)
                s16 = s8 + pltpu.roll(s8, 8, 0)
                totals.append(jnp.where(lane < 64, s8, s16)[16:])
        total = jnp.concatenate(totals, axis=1)
        lane = lax.broadcasted_iota(jnp.int32, (1, 256), 1)
        window = jnp.where(lane < 64, 2, jnp.where(lane < 128, 4, jnp.where(lane < 192, 8, 16)))
        position = sp * ROWS + lax.broadcasted_iota(jnp.int32, (16, 256), 0)
        early = total[:16] / jnp.minimum(position + 1, window).astype(F32)
        later = total[16:] * (1.0 / window.astype(F32))
        mixed_in = (jnp.concatenate([early, later], axis=0) - own).astype(BF)
        spread = (lax.rem(lax.broadcasted_iota(jnp.int32, (64, 256), 1), 64)
                  == lax.broadcasted_iota(jnp.int32, (64, 256), 0)).astype(F32).astype(BF)
        wide_mix = jnp.dot(pool_mix[...], spread, preferred_element_type=F32)
        same = (lax.div(lax.broadcasted_iota(jnp.int32, (256, 256), 0), 64)
                == lax.div(lax.broadcasted_iota(jnp.int32, (256, 256), 1), 64))
        block_mix = jnp.where(same, wide_mix, 0.0).astype(BF)
        grouped = jnp.dot(mixed_in, block_mix, preferred_element_type=F32)
        pooled[...] = (grouped * pool_scale[...]).astype(BF)

    with jax.named_scope("own_far"):
        mine(0, at(2))
        go(dn_args(0, at(2)))
        go(up_args(0, at(2)))
        go(dd_args(0, at(2)))
        go(dn_args(0, at(1)))

    with jax.named_scope("queries"):
        for s in range(2):
            arrived(qraw.at[s], q_recv.at[s])
            arrived(lamb.at[s], lam_recv.at[s])
            q = qraw[s]
            zero = jnp.zeros((64, ROWS), BF)
            qcat[s, 0] = jnp.concatenate([q[:64], zero], axis=0)
            qcat[s, 1] = jnp.concatenate([zero, q[64:]], axis=0)
            for m in range(2):
                top[s, m] = jnp.full((1, ROWS), NEG, F32)
                den[s, m] = jnp.zeros((1, ROWS), F32)
                acc[s, m] = jnp.zeros((128, ROWS), F32)

    def attend(zk, xk, first, masked):
        halves = [kv[zk, hf, xk] for hf in range(2)]
        keys = jnp.concatenate([h[:256] for h in halves], axis=0)
        vals = jnp.concatenate([h[256 + 128 * j:384 + 128 * j] for h in halves for j in range(2)], axis=1)
        tiles = [(s, m) for s in range(first, 2) for m in range(2)]

        def score(n):
            s, m = tiles[n]
            scores = jnp.dot(keys, qcat[s, m], preferred_element_type=F32)
            if masked and s == first:
                allowed = (lax.div(lax.broadcasted_iota(jnp.int32, (ROWS, ROWS), 0), SEG)
                           <= lax.div(lax.broadcasted_iota(jnp.int32, (ROWS, ROWS), 1), SEG))
                scores = jnp.where(allowed, scores, NEG)
            sbank[n % 2][...] = scores

        score(0)
        for n, (s, m) in enumerate(tiles):
            if n + 1 < len(tiles):
                score(n + 1)
            scores = sbank[n % 2][...]
            old = top[s, m]
            new = jnp.maximum(old, jnp.max(scores, axis=0, keepdims=True))
            probs = jnp.exp2(scores - new)
            shrink = jnp.exp2(old - new)
            top[s, m] = new
            den[s, m] = den[s, m] * shrink + jnp.sum(probs, axis=0, keepdims=True)
            acc[s, m] = acc[s, m] * shrink + jnp.dot(vals, probs.astype(BF), preferred_element_type=F32)

    def visit(rel, xk):
        zk = wrap(z + rel)
        arrived(kv.at[zk, 1 - c, xk], kv_recv.at[rel, 1 - c, xk])
        block = zk * 4 + xk

        @pl.when(block < qb[0])
        def _():
            attend(zk, xk, 0, False)

        @pl.when(block == qb[0])
        def _():
            attend(zk, xk, 0, True)

        @pl.when((block > qb[0]) & (block < qb[1]))
        def _():
            attend(zk, xk, 1, False)

        @pl.when(block == qb[1])
        def _():
            attend(zk, xk, 1, True)

    below, above = (0, 1, 3, 2), (0, 3, 2, 1)
    plan = ([(0, o) for o in below] + [p for i in range(4) for p in ((3, below[i]), (1, above[i]))]
            + [(2, o) for o in (0, 3, 1, 2)])

    def near(i):
        mine(3, at(below[i]))
        if i < 2:
            go(up_args(3, at(below[i])))
        go(dd_args(3, at(below[i])))
        mine(1, at(above[i]))
        if i in (1, 2):
            go(dn_args(1, at(above[i])))
        go(dd_args(1, at(above[i])))

    def far(i):
        for off in ((0, 3), (1, 2))[i]:
            mine(2, at(off))
            go(dd_args(2, at(off)))

    def pick(v, values):
        out_value = jnp.int32(values[0])
        for i, value in enumerate(values):
            if i:
                out_value = jnp.where(v == i, value, out_value)
        return out_value

    service = {0: (near, 0), 2: (near, 1), 5: (near, 2), 7: (near, 3), 10: (far, 0), 12: (far, 1)}

    with jax.named_scope("attend"):
        @pl.loop(0, 16)
        def _(v):
            for when, (serve, i) in service.items():
                @pl.when(v == when)
                def _():
                    serve(i)

            visit(pick(v, [p[0] for p in plan]), at(pick(v, [p[1] for p in plan])))

    ret_args = []
    with jax.named_scope("finish"):
        for s in range(2):
            o1 = acc[s, 0] / den[s, 0]
            o2 = acc[s, 1] / den[s, 1]
            blend = o1 - lamb[s][0:1, 0:1] * o2
            scaled = blend * lax.rsqrt(jnp.mean(blend * blend, axis=0, keepdims=True) + EPS)
            ao[s] = (scaled.T * head_gain[...] * 0.8).astype(BF)
            mine_h = lax.rem(x, 2)
            a = (ao.at[s], ab.at[mine_h], ret_send.at[s], ret_recv.at[mine_h], q_src[s])
            send_any(*a)
            ret_args.append(a)

    with jax.named_scope("drain"):
        remote(*rim_args).wait_send()
        for a in a2a_args + q_args:
            sent_any(*a)
        for off in range(4):
            remote(*up_args(0, at(off))).wait_send()
            remote(*dn_args(0, at(off))).wait_send()
            for rel in range(4):
                remote(*dd_args(rel, at(off))).wait_send()
        for i in range(2):
            remote(*up_args(3, at(below[i]))).wait_send()
            remote(*dn_args(1, at(above[i + 1]))).wait_send()

    for cp in w_loads:
        cp.wait()
    with jax.named_scope("home"):
        for hh in range(2):
            arrived(ab.at[hh], ret_recv.at[hh])

    order = [wrap(y + 2), wrap(y + 1), wrap(y - 1), y]

    def pd_args(h, k):
        return (pbuf.at[h, 2 * order[k] + 1 - c], dbuf.at[h, k], pd_send.at[h, k], pd_recv.at[h, k], partner)

    with jax.named_scope("project"):
        for h in range(2):
            feats = jnp.concatenate([pooled[...], ab[0], ab[1]], axis=1)
            term = jnp.dot(feats, w_out[:, 2048 * h:2048 * h + 2048], preferred_element_type=F32)
            pbuf[h] = term.astype(BF).reshape(8, 64, 2048)
            for k in range(4):
                go(pd_args(h, k))

    def chip_sum(h, k):
        arrived(dbuf.at[h, k], pd_recv.at[h, k])
        return pbuf[h, 2 * order[k] + c].astype(F32) + dbuf[h, k].astype(F32)

    A, B = 0, 1
    y_args = [
        (sbuf.at[0], relay.at[0], y_send.at[0], y_recv.at[0], y_up),
        (sbuf.at[1], relay.at[1], y_send.at[1], y_recv.at[1], y_dn),
        (sbuf.at[2], fin.at[0, B], y_send.at[2], y_recv.at[2], y_up),
        (sbuf.at[3], fin.at[1, A], y_send.at[3], y_recv.at[3], y_dn),
        (sbuf.at[4], fin.at[0, A], y_send.at[4], y_recv.at[4], y_up),
        (sbuf.at[5], fin.at[1, B], y_send.at[5], y_recv.at[5], y_dn),
    ]

    def y_go(i, value):
        sbuf[i] = value.astype(BF)
        remote(*y_args[i]).start()

    with jax.named_scope("y_first"):
        y_go(0, chip_sum(A, 0))
        y_go(1, chip_sum(B, 0))
        y_go(3, chip_sum(A, 2))
        y_go(2, chip_sum(B, 1))
    with jax.named_scope("y_relay"):
        up = chip_sum(A, 1)
        arrived(relay.at[0], y_recv.at[0])
        y_go(4, up + relay[0].astype(F32))
        dn = chip_sum(B, 2)
        arrived(relay.at[1], y_recv.at[1])
        y_go(5, dn + relay[1].astype(F32))

    with jax.named_scope("y_last"):
        arrived(fin.at[0, B], y_recv.at[2])
        arrived(fin.at[1, A], y_recv.at[3])
        arrived(fin.at[0, A], y_recv.at[4])
        arrived(fin.at[1, B], y_recv.at[5])
        for h in range(2):
            whole = chip_sum(h, 3) + fin[0, h].astype(F32) + fin[1, h].astype(F32)
            out[:, 2048 * h:2048 * h + 2048] = whole.astype(BF)

    for a in ret_args:
        sent_any(*a)
    for h in range(2):
        for k in range(4):
            remote(*pd_args(h, k)).wait_send()
    for a in y_args:
        remote(*a).wait_send()


def body(tokens, norm_gain, w_pool_in, w_query, w_key, w_value, pool_mix, pool_scale, lam, head_gain,
         pool_proj, attn_proj):
    sd = jax.ShapeDtypeStruct
    dma = pltpu.SemaphoreType.DMA
    return pl.pallas_call(
        mixer_kernel,
        out_shape=sd((64, WIDE), BF),
        in_specs=[ANY, VM, ANY, ANY, ANY, ANY, SM, VM, VM, VM, ANY, ANY],
        out_specs=VM,
        scratch_shapes=[
            pltpu.VMEM((ROWS, WIDE), BF),
            pltpu.VMEM((ROWS, WIDE), BF),
            pltpu.VMEM((4, WIDE, 256), BF),
            pltpu.VMEM((2, 2, 512, 128), BF),
            pltpu.VMEM((2, 128, ROWS), BF),
            pltpu.VMEM((ROWS, 256), BF),
            pltpu.VMEM((2, 8, 128), F32),
            pltpu.VMEM((4, 2, 4, 512, 128), BF),
            pltpu.VMEM((2, 128, ROWS), BF),
            pltpu.VMEM((2, 2, 128, ROWS), BF),
            pltpu.VMEM((2, 8, 128), F32),
            pltpu.VMEM((16, 256), BF),
            pltpu.VMEM((2, 2, 128, ROWS), F32),
            pltpu.VMEM((2, 2, 1, ROWS), F32),
            pltpu.VMEM((2, 2, 1, ROWS), F32),
            pltpu.VMEM((ROWS, ROWS), F32),
            pltpu.VMEM((ROWS, ROWS), F32),
            pltpu.VMEM((2, ROWS, 128), BF),
            pltpu.VMEM((2, ROWS, 128), BF),
            pltpu.VMEM((ROWS, 256), BF),
            pltpu.VMEM((512, WIDE), BF),
            pltpu.VMEM((2, 8, 64, 2048), BF),
            pltpu.VMEM((2, 4, 64, 2048), BF),
            pltpu.VMEM((6, 64, 2048), BF),
            pltpu.VMEM((2, 64, 2048), BF),
            pltpu.VMEM((2, 2, 64, 2048), BF),
            dma((4,)), dma((6,)), dma((2, 2)), dma((4, 2, 4)), dma((2,)), dma((2,)), dma((2,)), dma((2,)),
            dma, dma, dma((2, 4)), dma((2, 4)), dma((4, 4)), dma((2,)), dma((2,)),
            dma((2, 4)), dma((2, 4)), dma((6,)), dma((6,)),
        ],
        compiler_params=pltpu.CompilerParams(vmem_limit_bytes=67043328, collective_id=0, has_side_effects=True),
        name="mixer",
    )(tokens, norm_gain.reshape(1, WIDE), w_key, w_value, w_query, w_pool_in, lam, pool_mix.reshape(256, 64),
      pool_scale.reshape(1, 256), head_gain.reshape(1, 128), pool_proj, attn_proj)


def solution(mesh):
    return jax.shard_map(
        body,
        mesh=mesh,
        in_specs=(P("sp", None), P(), P(None, "tp"), P(None, "tp"), P(None, "tp"), P(None, "tp"),
                  P("tp", None, None), P("tp"), P("tp"), P(), P("tp", None), P("tp", None)),
        out_specs=P(("sp", "tp"), None),
        check_vma=False,
    )
```

```python
import jax
import jax.numpy as jnp
from jax import lax
from jax.experimental import pallas as pl
from jax.experimental.pallas import tpu as pltpu
from jax.sharding import PartitionSpec as P

EPS = 1e-6
NEG = -1e30
LOG2E = 1.4426950408889634
ROWS = 512
WIDE = 4096
SEG = 64
BF = jnp.bfloat16
F32 = jnp.float32
MESH_ID = pl.DeviceIdType.MESH
OUTER = ((2, 3, 0, 1), (0, 3, 1, 2), (3, 2, 1, 0), (1, 0, 3, 2))
INNER = ((0, 2, 1, 3), (2, 1, 3, 0), (1, 0, 3, 2), (3, 2, 1, 0))


def pick(at, values):
    packed = sum(value << (2 * i) for i, value in enumerate(values))
    packed = packed - (1 << 32) if packed >= 1 << 31 else packed
    return lax.shift_right_logical(jnp.int32(packed), 2 * at) & 3


def flat(table):
    return [value for row in table for value in row]


def inverse(table):
    return [row.index(value) for row in table for value in range(4)]
ANY = pl.BlockSpec(memory_space=pl.ANY)
VM = pl.BlockSpec(memory_space=pltpu.VMEM)
SM = pl.BlockSpec(memory_space=pltpu.SMEM)


def mixer_kernel(tok, gain, w_k, w_v, w_q, w_p, lam, pool_mix, pool_scale, head_gain, pool_proj, attn_proj,
                 out,
                 raw, normed, wts, kv_in, q_in, pool_in, lam_in, kv, qraw, qcat, lamb, rim, acc, top, den, sbank_a, sbank_b, smax, x_relay, ao, ab, pooled, w_out, pbuf, dbuf, sbuf, relay, fin,
                 tok_sem, w_sem, x_recv, pass_send, a2a_send, kv_recv, q_send, q_recv, lam_send, lam_recv, rim_send, rim_recv,
                 zp_send, zm_send, dd_send, ret_send, ret_recv, pd_send, pd_recv, y_send, y_recv):
    sbank = (sbank_a, sbank_b)
    sp = lax.axis_index("sp")
    tp = lax.axis_index("tp")
    z, x = lax.div(sp, 4), lax.rem(sp, 4)
    y, c = lax.div(tp, 2), lax.rem(tp, 2)

    def wrap(i):
        return lax.rem(i + 4, 4)

    def dev(zz, xx, cc):
        return (zz * 4 + xx, y * 2 + cc)

    def at(off):
        return lax.rem(x + off, 4)

    me = (sp, tp)

    def is_me(d):
        return (d[0] == sp) & (d[1] == tp)

    core_src = lax.div(x, 2)
    outer_row = (z == 0) | (z == 3)
    place = jnp.where(z < 2, x, 3 - x)
    cq = jnp.where(outer_row, 0, 1)
    sq = lax.div(z, 2)
    a_here, b_here = pick(x * 4 + z, flat(OUTER)), pick(x * 4 + z, flat(INNER))
    qb = [jnp.where(c == 0, a_here, 4 + b_here), jnp.where(c == 0, 15 - a_here, 11 - b_here)]
    partner = dev(z, x, 1 - c)
    z_up, z_dn = dev(wrap(z + 1), x, c), dev(wrap(z - 1), x, c)
    y_up = (sp, wrap(y + 1) * 2 + c)
    y_dn = (sp, wrap(y - 1) * 2 + c)
    nxt = (lax.rem(sp + 1, 16), tp)
    prv = (lax.rem(sp + 15, 16), tp)
    a2a_dst = [[dev(z, 2 * c + hh, hf) for hf in range(2)] for hh in range(2)]
    q_dst = []
    for hh in range(2):
        spot = (2 * c + hh) * 4 + place
        q_dst.append(dev(jnp.where(outer_row, pick(spot, inverse(OUTER)), pick(spot, inverse(INNER))), 2 * c + hh, cq))
    q_src = [dev(lax.div(qb[s], 4), lax.rem(qb[s], 4), core_src) for s in range(2)]

    def load(src, dst, sem):
        cp = pltpu.make_async_copy(src, dst, sem)
        cp.start()
        return cp

    tok_loads = [load(tok.at[pl.ds(r * 128, 128)], raw.at[pl.ds(r * 128, 128)], tok_sem.at[r]) for r in range(4)]
    in_loads = []

    barrier = pltpu.get_barrier_semaphore()

    def greet(d):
        pl.semaphore_signal(barrier, inc=1, device_id=d, device_id_type=MESH_ID)

    behind, beyond = jnp.where(c == 0, at(3), at(1)), jnp.where(c == 0, at(1), at(3))
    greeted = [dev(z, at(off), core_src) for off in (0, 1, 3)] + [dev(z, behind, lax.div(beyond, 2)), dev(z, behind, c)]
    greeted = greeted + q_src + q_dst + [z_up, z_dn, partner, y_up, y_dn, prv]
    for d in greeted:
        greet(d)

    def remote(src, dst, ssem, rsem, d):
        return pltpu.make_async_remote_copy(src_ref=src, dst_ref=dst, send_sem=ssem, recv_sem=rsem,
                                            device_id=d, device_id_type=MESH_ID)

    def send_any(src, dst, ssem, rsem, d):
        @pl.when(is_me(d))
        def _():
            pltpu.make_async_copy(src, dst, rsem).start()

        @pl.when(jnp.logical_not(is_me(d)))
        def _():
            remote(src, dst, ssem, rsem, d).start()

    def sent_any(src, dst, ssem, rsem, d):
        @pl.when(jnp.logical_not(is_me(d)))
        def _():
            remote(src, dst, ssem, rsem, d).wait_send()

    def arrived(dst, rsem):
        pltpu.make_async_copy(dst, dst, rsem).wait()

    for hh in range(2):
        lam_in[hh] = jnp.full((8, 128), lam[hh], F32)
    with jax.named_scope("norm"):
        for r in range(4):
            tok_loads[r].wait()
            in_loads.append(load((w_q, w_k, w_v, w_p)[r], wts.at[r], w_sem.at[r]))

            @pl.loop(0, 8, unroll=4)
            def _(i):
                rows = pl.ds(pl.multiple_of(r * 128 + i * 16, 16), 16)
                wide = raw[rows].astype(F32)
                scale = lax.rsqrt(jnp.mean(wide * wide, axis=-1, keepdims=True) + EPS)
                normed[rows] = (wide * scale * gain[...]).astype(BF)

    def product(i):
        return jnp.dot(normed[...], wts[i], preferred_element_type=F32)

    def halves(i, finish_half):
        for r in range(2):
            rows = slice(256 * r, 256 * r + 256)
            finish_half(rows, jnp.dot(normed[rows], wts[i], preferred_element_type=F32))

    with jax.named_scope("query"):
        in_loads[0].wait()

        def query_half(rows, value):
            value = value * (0.125 * LOG2E)
            for hh in range(2):
                q_in[hh, :, rows] = value[:, 128 * hh:128 * hh + 128].T.astype(BF)

        halves(0, query_half)
    pl.semaphore_wait(barrier, len(greeted))
    q_args = []
    for hh in range(2):
        q_args.append((q_in.at[hh], qraw.at[sq], q_send.at[hh], q_recv.at[sq], q_dst[hh]))
        q_args.append((lam_in.at[hh], lamb.at[sq], lam_send.at[hh], lam_recv.at[sq], q_dst[hh]))
    for a in q_args:
        send_any(*a)

    with jax.named_scope("keys_values"):
        for i in range(1, 3):
            in_loads[i].wait()
        w_loads = [load(pool_proj, w_out.at[pl.ds(0, 256)], w_sem.at[4]),
                   load(attn_proj, w_out.at[pl.ds(256, 256)], w_sem.at[5])]
        keys = product(1).astype(BF)
        values = product(2)
        for hh in range(2):
            for hf in range(2):
                kv_in[hh, hf, 0:256] = keys[256 * hf:256 * hf + 256, 128 * hh:128 * hh + 128]
                for j in range(2):
                    first = 256 * hf + 128 * j
                    tile = values[first:first + 128, 128 * hh:128 * hh + 128]
                    kv_in[hh, hf, 256 + 128 * j:384 + 128 * j] = tile.T.astype(BF)

    a2a_args = []
    for hh in range(2):
        for hf in range(2):
            a2a_args.append((kv_in.at[hh, hf], kv.at[z, hf, x], a2a_send.at[hh, hf], kv_recv.at[0, hf, x],
                             a2a_dst[hh][hf]))

    def hop_args(hh, hf):
        return (kv_in.at[hh, hf], x_relay, a2a_send.at[hh, hf], x_recv, dev(z, at(1 if hf == 0 else 3), hf))

    for hh in range(2):
        is_across = wrap(2 * c + hh - x) == 2

        @pl.when(jnp.logical_not(is_across))
        def _():
            for hf in range(2):
                send_any(*a2a_args[2 * hh + hf])

    for hh in range(2):
        is_across = wrap(2 * c + hh - x) == 2

        @pl.when(is_across)
        def _():
            for hf in range(2):
                remote(*hop_args(hh, hf)).start()

    hop_from = jnp.where(c == 0, at(3), at(1))
    pass_args = (x_relay, kv.at[z, c, hop_from], pass_send, kv_recv.at[0, c, hop_from],
                 dev(z, jnp.where(c == 0, at(1), at(3)), c))


    def dd_args(rel, xk):
        piece = kv.at[wrap(z + rel), c, xk]
        return (piece, piece, dd_send.at[rel, xk], kv_recv.at[rel, c, xk], partner)

    def up_args(rel, xk):
        piece = kv.at[wrap(z + rel), c, xk]
        return (piece, piece, zp_send.at[rel & 1, xk], kv_recv.at[(rel + 3) % 4, c, xk], z_up)

    def dn_args(rel, xk):
        piece = kv.at[wrap(z + rel), c, xk]
        return (piece, piece, zm_send.at[rel & 1, xk], kv_recv.at[(rel + 1) % 4, c, xk], z_dn)

    def mine(rel, xk):
        arrived(kv.at[wrap(z + rel), c, xk], kv_recv.at[rel, c, xk])

    def go(args):
        remote(*args).start()

    mine(0, at(0))
    go(up_args(0, at(0)))
    go(dn_args(0, at(0)))
    go(dd_args(0, at(0)))

    with jax.named_scope("pool_in"):
        in_loads[3].wait()

        def pool_half(rows, value):
            pool_in[rows] = value.astype(BF)

        halves(3, pool_half)
    rim_args = (pool_in.at[pl.ds(ROWS - 16, 16)], rim, rim_send, rim_recv, nxt)
    remote(*rim_args).start()

    with jax.named_scope("own_near"):
        mine(0, at(1))
        go(up_args(0, at(1)))
        go(dd_args(0, at(1)))
        mine(0, at(3))
        go(dn_args(0, at(3)))
        go(up_args(0, at(3)))
        go(dd_args(0, at(3)))
        arrived(x_relay, x_recv)
        go(pass_args)

    with jax.named_scope("queries"):
        for s in range(2):
            arrived(qraw.at[s], q_recv.at[s])
            arrived(lamb.at[s], lam_recv.at[s])
            q = qraw[s]
            zero = jnp.zeros((64, ROWS), BF)
            qcat[s, 0] = jnp.concatenate([q[:64], zero], axis=0)
            qcat[s, 1] = jnp.concatenate([zero, q[64:]], axis=0)
            for m in range(2):
                top[s, m] = jnp.full((1, ROWS), NEG, F32)
                den[s, m] = jnp.zeros((1, ROWS), F32)
                acc[s, m] = jnp.zeros((128, ROWS), F32)

    def score(bank, zk, xk, s, m):
        keys = jnp.concatenate([kv[zk, hf, xk, 0:256] for hf in range(2)], axis=0)
        scores = jnp.dot(keys, qcat[s, m], preferred_element_type=F32)
        sbank[bank][...] = scores
        smax[bank] = jnp.max(scores, axis=0, keepdims=True)

    def weigh(bank, zk, xk, s, m, masked):
        vals = jnp.concatenate([kv[zk, hf, xk, 256 + 128 * j:384 + 128 * j] for hf in range(2) for j in range(2)],
                               axis=1)
        scores = sbank[bank][...]
        peak = smax[bank]
        if masked:
            allowed = (lax.div(lax.broadcasted_iota(jnp.int32, (ROWS, ROWS), 0), SEG)
                       <= lax.div(lax.broadcasted_iota(jnp.int32, (ROWS, ROWS), 1), SEG))
            scores = jnp.where(allowed, scores, NEG)
            peak = jnp.max(scores, axis=0, keepdims=True)
        old = top[s, m]
        new = jnp.maximum(old, peak)
        probs = jnp.exp2(scores - new)
        shrink = jnp.exp2(old - new)
        top[s, m] = new
        den[s, m] = den[s, m] * shrink + jnp.sum(probs, axis=0, keepdims=True)
        acc[s, m] = acc[s, m] * shrink + jnp.dot(vals, probs.astype(BF), preferred_element_type=F32)

    def attend(here, ahead, slots, masked):
        tiles = [(s, m) for s in slots for m in range(2)]
        for n, (s, m) in enumerate(tiles):
            if n + 1 < len(tiles):
                score((n + 1) % 2, *here, *tiles[n + 1])
            else:
                score(0, *ahead, 1, 0)
            weigh(n % 2, *here, s, m, masked == s)

    def joined(rel, xk):
        arrived(kv.at[wrap(z + rel), 1 - c, xk], kv_recv.at[rel, 1 - c, xk])

    def visit(here, ahead):
        block = here[0] * 4 + here[1]

        @pl.when(block <= qb[1])
        def _():
            @pl.when(block > qb[0])
            def _():
                @pl.when(block < qb[1])
                def _():
                    attend(here, ahead, (1,), None)

                @pl.when(block == qb[1])
                def _():
                    attend(here, ahead, (1,), 1)

            @pl.when(block <= qb[0])
            def _():
                @pl.when(block < qb[0])
                def _():
                    attend(here, ahead, (1, 0), None)

                @pl.when(block == qb[0])
                def _():
                    attend(here, ahead, (1, 0), 0)

        @pl.when(block > qb[1])
        def _():
            score(0, *ahead, 1, 0)

    below, above = (0, 1, 3, 2), (0, 3, 2, 1)
    plan = ([(0, o) for o in below] + [p for i in range(4) for p in ((3, below[i]), (1, above[i]))]
            + [(2, o) for o in (0, 3, 1, 2)])

    def near(i):
        mine(3, at(below[i]))
        if i < 2:
            go(up_args(3, at(below[i])))
        go(dd_args(3, at(below[i])))
        mine(1, at(above[i]))
        if i in (1, 2):
            go(dn_args(1, at(above[i])))
        go(dd_args(1, at(above[i])))

    def far(i):
        for off in ((0, 3), (1, 2))[i]:
            mine(2, at(off))
            go(dd_args(2, at(off)))

    def pooling(_):
        arrived(rim, rim_recv)
        edge = jnp.where(sp == 0, 0.0, rim[...].astype(F32))
        own = pool_in[...].astype(F32)
        lane = lax.broadcasted_iota(jnp.int32, (1, 128), 1)
        totals = []
        for side in range(2):
            cols = slice(128 * side, 128 * side + 128)
            line = jnp.concatenate([edge[:, cols], own[:, cols]], axis=0)
            s2 = line + pltpu.roll(line, 1, 0)
            s4 = s2 + pltpu.roll(s2, 2, 0)
            if side == 0:
                totals.append(jnp.where(lane < 64, s2, s4)[16:])
            else:
                s8 = s4 + pltpu.roll(s4, 4, 0)
                s16 = s8 + pltpu.roll(s8, 8, 0)
                totals.append(jnp.where(lane < 64, s8, s16)[16:])
        total = jnp.concatenate(totals, axis=1)
        lane = lax.broadcasted_iota(jnp.int32, (1, 256), 1)
        window = jnp.where(lane < 64, 2, jnp.where(lane < 128, 4, jnp.where(lane < 192, 8, 16)))
        position = sp * ROWS + lax.broadcasted_iota(jnp.int32, (16, 256), 0)
        early = total[:16] / jnp.minimum(position + 1, window).astype(F32)
        later = total[16:] * (1.0 / window.astype(F32))
        mixed_in = (jnp.concatenate([early, later], axis=0) - own).astype(BF)
        spread = (lax.rem(lax.broadcasted_iota(jnp.int32, (64, 256), 1), 64)
                  == lax.broadcasted_iota(jnp.int32, (64, 256), 0)).astype(F32).astype(BF)
        wide_mix = jnp.dot(pool_mix[...], spread, preferred_element_type=F32)
        same = (lax.div(lax.broadcasted_iota(jnp.int32, (256, 256), 0), 64)
                == lax.div(lax.broadcasted_iota(jnp.int32, (256, 256), 1), 64))
        block_mix = jnp.where(same, wide_mix, 0.0).astype(BF)
        grouped = jnp.dot(mixed_in, block_mix, preferred_element_type=F32)
        pooled[...] = (grouped * pool_scale[...]).astype(BF)

    def own_far(_):
        mine(0, at(2))
        go(dn_args(0, at(2)))
        go(up_args(0, at(2)))
        go(dd_args(0, at(2)))
        go(dn_args(0, at(1)))

    service = {0: (near, 0), 2: (own_far, 0), 3: (near, 1), 5: (near, 2), 7: (near, 3), 9: (pooling, 0), 10: (far, 0),
               12: (far, 1)}

    mine_h = lax.rem(x, 2)
    ret_args = [(ao.at[s], ab.at[mine_h], ret_send.at[s], ret_recv.at[mine_h], q_src[s]) for s in range(2)]

    def finish(s):
        o1 = acc[s, 0] / den[s, 0]
        o2 = acc[s, 1] / den[s, 1]
        blend = o1 - lamb[s][0:1, 0:1] * o2
        scaled = blend * lax.rsqrt(jnp.mean(blend * blend, axis=0, keepdims=True) + EPS)
        ao[s] = (scaled.T * head_gain[...] * 0.8).astype(BF)
        send_any(*ret_args[s])

    soon = wrap(z + 2) * 4 > qb[0]

    with jax.named_scope("attend"):
        joined(0, at(0))
        score(0, z, at(0), 1, 0)

        @pl.loop(0, 16)
        def _(v):
            @pl.when(pick(v, [int(i in service) for i in range(16)]) == 1)
            def _():
                for when, (serve, i) in service.items():
                    @pl.when(v == when)
                    def _():
                        with jax.named_scope(f"serve{when}"):
                            serve(i)

            @pl.when((v == 12) & soon)
            def _():
                finish(0)

            follow = jnp.minimum(v + 1, 15)
            rel, nrel = (pick(i, [p[0] for p in plan]) for i in (v, follow))
            xk, nxk = (at(pick(i, [p[1] for p in plan])) for i in (v, follow))

            @pl.when(v < 15)
            def _():
                with jax.named_scope("join"):
                    joined(nrel, nxk)

            with jax.named_scope("visit"):
                visit((wrap(z + rel), xk), (wrap(z + nrel), nxk))

    with jax.named_scope("finish"):
        finish(1)

        @pl.when(jnp.logical_not(soon))
        def _():
            finish(0)

    with jax.named_scope("drain"):
        remote(*rim_args).wait_send()
        for a in a2a_args + q_args:
            sent_any(*a)
        remote(*pass_args).wait_send()
        for off in range(4):
            remote(*up_args(0, at(off))).wait_send()
            remote(*dn_args(0, at(off))).wait_send()
            for rel in range(4):
                remote(*dd_args(rel, at(off))).wait_send()
        for i in range(2):
            remote(*up_args(3, at(below[i]))).wait_send()
            remote(*dn_args(1, at(above[i + 1]))).wait_send()

    for cp in w_loads:
        cp.wait()
    with jax.named_scope("home"):
        for hh in range(2):
            arrived(ab.at[hh], ret_recv.at[hh])

    order = [wrap(y + 2), wrap(y + 1), wrap(y - 1), y]

    def pd_args(h, k):
        return (pbuf.at[h, 2 * order[k] + 1 - c], dbuf.at[h, k], pd_send.at[h, k], pd_recv.at[h, k], partner)

    def project(h):
        feats = jnp.concatenate([pooled[...], ab[0], ab[1]], axis=1)
        term = jnp.dot(feats, w_out[:, 1024 * h:1024 * h + 1024], preferred_element_type=F32)
        pbuf[h] = term.astype(BF).reshape(8, 64, 1024)
        for k in range(4):
            go(pd_args(h, k))

    def chip_sum(h, k):
        arrived(dbuf.at[h, k], pd_recv.at[h, k])
        return pbuf[h, 2 * order[k] + c].astype(F32) + dbuf[h, k].astype(F32)

    def relay_args(h):
        return (sbuf.at[0, h], relay.at[h], y_send.at[0, h], y_recv.at[0, h], y_up if h < 2 else y_dn)

    def up_sum_args(h):
        return (sbuf.at[1, h], fin.at[0, h], y_send.at[1, h], y_recv.at[1, h], y_up)

    def dn_sum_args(h):
        return (sbuf.at[2, h], fin.at[1, h], y_send.at[2, h], y_recv.at[2, h], y_dn)

    def put(i, h, value, args):
        sbuf[i, h] = value.astype(BF)
        go(args)

    def start_relay(h):
        put(0, h, chip_sum(h, 0), relay_args(h))

    def direct(h):
        if h < 2:
            put(2, h, chip_sum(h, 2), dn_sum_args(h))
        else:
            put(1, h, chip_sum(h, 1), up_sum_args(h))

    def relayed(h):
        own_sum = chip_sum(h, 1 if h < 2 else 2)
        arrived(relay.at[h], y_recv.at[0, h])
        value = own_sum + relay[h].astype(F32)
        if h < 2:
            put(1, h, value, up_sum_args(h))
        else:
            put(2, h, value, dn_sum_args(h))

    with jax.named_scope("out_first"):
        project(0)
        project(2)
        start_relay(0)
        project(1)
        start_relay(2)
        project(3)
        start_relay(1)
        start_relay(3)
    with jax.named_scope("out_direct"):
        for h in (0, 2, 1, 3):
            direct(h)
    with jax.named_scope("out_relayed"):
        for h in (0, 2, 1, 3):
            relayed(h)
    with jax.named_scope("out_last"):
        for h in (2, 0, 3, 1):
            own_sum = chip_sum(h, 3)
            arrived(fin.at[0, h], y_recv.at[1, h])
            arrived(fin.at[1, h], y_recv.at[2, h])
            whole = own_sum + fin[0, h].astype(F32) + fin[1, h].astype(F32)
            out[:, 1024 * h:1024 * h + 1024] = whole.astype(BF)

    for a in ret_args:
        sent_any(*a)
    for h in range(4):
        for k in range(4):
            remote(*pd_args(h, k)).wait_send()
        remote(*relay_args(h)).wait_send()
        remote(*up_sum_args(h)).wait_send()
        remote(*dn_sum_args(h)).wait_send()


def body(tokens, norm_gain, w_pool_in, w_query, w_key, w_value, pool_mix, pool_scale, lam, head_gain,
         pool_proj, attn_proj):
    sd = jax.ShapeDtypeStruct
    dma = pltpu.SemaphoreType.DMA
    return pl.pallas_call(
        mixer_kernel,
        out_shape=sd((64, WIDE), BF),
        in_specs=[ANY, VM, ANY, ANY, ANY, ANY, SM, VM, VM, VM, ANY, ANY],
        out_specs=VM,
        scratch_shapes=[
            pltpu.VMEM((ROWS, WIDE), BF),
            pltpu.VMEM((ROWS, WIDE), BF),
            pltpu.VMEM((4, WIDE, 256), BF),
            pltpu.VMEM((2, 2, 512, 128), BF),
            pltpu.VMEM((2, 128, ROWS), BF),
            pltpu.VMEM((ROWS, 256), BF),
            pltpu.VMEM((2, 8, 128), F32),
            pltpu.VMEM((4, 2, 4, 512, 128), BF),
            pltpu.VMEM((2, 128, ROWS), BF),
            pltpu.VMEM((2, 2, 128, ROWS), BF),
            pltpu.VMEM((2, 8, 128), F32),
            pltpu.VMEM((16, 256), BF),
            pltpu.VMEM((2, 2, 128, ROWS), F32),
            pltpu.VMEM((2, 2, 1, ROWS), F32),
            pltpu.VMEM((2, 2, 1, ROWS), F32),
            pltpu.VMEM((ROWS, ROWS), F32),
            pltpu.VMEM((ROWS, ROWS), F32),
            pltpu.VMEM((2, 1, ROWS), F32),
            pltpu.VMEM((512, 128), BF),
            pltpu.VMEM((2, ROWS, 128), BF),
            pltpu.VMEM((2, ROWS, 128), BF),
            pltpu.VMEM((ROWS, 256), BF),
            pltpu.VMEM((512, WIDE), BF),
            pltpu.VMEM((4, 8, 64, 1024), BF),
            pltpu.VMEM((4, 4, 64, 1024), BF),
            pltpu.VMEM((3, 4, 64, 1024), BF),
            pltpu.VMEM((4, 64, 1024), BF),
            pltpu.VMEM((2, 4, 64, 1024), BF),
            dma((4,)), dma((6,)), dma, dma, dma((2, 2)), dma((4, 2, 4)), dma((2,)), dma((2,)), dma((2,)), dma((2,)),
            dma, dma, dma((2, 4)), dma((2, 4)), dma((4, 4)), dma((2,)), dma((2,)),
            dma((4, 4)), dma((4, 4)), dma((3, 4)), dma((3, 4)),
        ],
        compiler_params=pltpu.CompilerParams(vmem_limit_bytes=67043328, collective_id=0, has_side_effects=True),
        name="mixer",
    )(tokens, norm_gain.reshape(1, WIDE), w_key, w_value, w_query, w_pool_in, lam, pool_mix.reshape(256, 64),
      pool_scale.reshape(1, 256), head_gain.reshape(1, 128), pool_proj, attn_proj)


def solution(mesh):
    return jax.shard_map(
        body,
        mesh=mesh,
        in_specs=(P("sp", None), P(), P(None, "tp"), P(None, "tp"), P(None, "tp"), P(None, "tp"),
                  P("tp", None, None), P("tp"), P("tp"), P(), P("tp", None), P("tp", None)),
        out_specs=P(("sp", "tp"), None),
        check_vma=False,
    )
```

```python
import jax
import jax.numpy as jnp
from jax import lax
from jax.experimental import pallas as pl
from jax.experimental.pallas import tpu as pltpu
from jax.sharding import PartitionSpec as P

EPS = 1e-6
NEG = -1e30
LOG2E = 1.4426950408889634
ROWS = 512
WIDE = 4096
SEG = 64
BF = jnp.bfloat16
F32 = jnp.float32
MESH_ID = pl.DeviceIdType.MESH
OUTER = ((2, 3, 0, 1), (0, 3, 1, 2), (3, 2, 1, 0), (1, 0, 3, 2))
INNER = ((0, 2, 1, 3), (2, 1, 3, 0), (1, 0, 3, 2), (3, 2, 1, 0))


def pick(at, values):
    packed = sum(value << (2 * i) for i, value in enumerate(values))
    packed = packed - (1 << 32) if packed >= 1 << 31 else packed
    return lax.shift_right_logical(jnp.int32(packed), 2 * at) & 3


def flat(table):
    return [value for row in table for value in row]


def inverse(table):
    return [row.index(value) for row in table for value in range(4)]
ANY = pl.BlockSpec(memory_space=pl.ANY)


def mixer_kernel(tok, gain_in, w_k, w_v, w_q, w_p, lam_hbm, mix_in, scale_in, head_gain_in, pool_proj, attn_proj,
                 out,
                 gain, lam, pool_mix, pool_scale, head_gain, out_buf, small_sem, out_sem, raw, normed, wts, kv_in, q_in, pool_in, lam_in, kv, qraw, qcat, lamb, rim, acc, top, den, sbank_a, sbank_b, smax, x_relay, ao, ab, pooled, w_out, pbuf, dbuf, sbuf, relay, fin,
                 tok_sem, w_sem, x_recv, pass_send, a2a_send, kv_recv, q_send, q_recv, lam_send, lam_recv, rim_send, rim_recv,
                 zp_send, zm_send, dd_send, ret_send, ret_recv, pd_send, pd_recv, y_send, y_recv):
    sbank = (sbank_a, sbank_b)
    sp = lax.axis_index("sp")
    tp = lax.axis_index("tp")
    z, x = lax.div(sp, 4), lax.rem(sp, 4)
    y, c = lax.div(tp, 2), lax.rem(tp, 2)

    def wrap(i):
        return lax.rem(i + 4, 4)

    def dev(zz, xx, cc):
        return (zz * 4 + xx, y * 2 + cc)

    def at(off):
        return lax.rem(x + off, 4)

    me = (sp, tp)

    def is_me(d):
        return (d[0] == sp) & (d[1] == tp)

    core_src = lax.div(x, 2)
    outer_row = (z == 0) | (z == 3)
    place = jnp.where(z < 2, x, 3 - x)
    cq = jnp.where(outer_row, 0, 1)
    sq = lax.div(z, 2)
    a_here, b_here = pick(x * 4 + z, flat(OUTER)), pick(x * 4 + z, flat(INNER))
    qb = [jnp.where(c == 0, a_here, 4 + b_here), jnp.where(c == 0, 15 - a_here, 11 - b_here)]
    partner = dev(z, x, 1 - c)
    z_up, z_dn = dev(wrap(z + 1), x, c), dev(wrap(z - 1), x, c)
    y_up = (sp, wrap(y + 1) * 2 + c)
    y_dn = (sp, wrap(y - 1) * 2 + c)
    nxt = (lax.rem(sp + 1, 16), tp)
    prv = (lax.rem(sp + 15, 16), tp)
    a2a_dst = [[dev(z, 2 * c + hh, hf) for hf in range(2)] for hh in range(2)]
    q_dst = []
    for hh in range(2):
        spot = (2 * c + hh) * 4 + place
        q_dst.append(dev(jnp.where(outer_row, pick(spot, inverse(OUTER)), pick(spot, inverse(INNER))), 2 * c + hh, cq))
    q_src = [dev(lax.div(qb[s], 4), lax.rem(qb[s], 4), core_src) for s in range(2)]

    def load(src, dst, sem):
        cp = pltpu.make_async_copy(src, dst, sem)
        cp.start()
        return cp

    tok_loads = [load(tok.at[pl.ds(r * 128, 128)], raw.at[pl.ds(r * 128, 128)], tok_sem.at[r]) for r in range(4)]
    small = [load(src, dst, small_sem.at[i]) for i, (src, dst) in enumerate(
        ((gain_in, gain), (lam_hbm, lam), (mix_in, pool_mix), (scale_in, pool_scale), (head_gain_in, head_gain)))]
    in_loads = []

    barrier = pltpu.get_barrier_semaphore()

    def greet(d):
        pl.semaphore_signal(barrier, inc=1, device_id=d, device_id_type=MESH_ID)

    behind, beyond = jnp.where(c == 0, at(3), at(1)), jnp.where(c == 0, at(1), at(3))
    greeted = [dev(z, at(off), core_src) for off in (0, 1, 3)] + [dev(z, behind, lax.div(beyond, 2)), dev(z, behind, c)]
    greeted = greeted + q_src + q_dst + [z_up, z_dn, partner, y_up, y_dn, prv]
    for d in greeted:
        greet(d)

    def remote(src, dst, ssem, rsem, d):
        return pltpu.make_async_remote_copy(src_ref=src, dst_ref=dst, send_sem=ssem, recv_sem=rsem,
                                            device_id=d, device_id_type=MESH_ID)

    def send_any(src, dst, ssem, rsem, d):
        @pl.when(is_me(d))
        def _():
            pltpu.make_async_copy(src, dst, rsem).start()

        @pl.when(jnp.logical_not(is_me(d)))
        def _():
            remote(src, dst, ssem, rsem, d).start()

    def sent_any(src, dst, ssem, rsem, d):
        @pl.when(jnp.logical_not(is_me(d)))
        def _():
            remote(src, dst, ssem, rsem, d).wait_send()

    def arrived(dst, rsem):
        pltpu.make_async_copy(dst, dst, rsem).wait()

    small[0].wait()
    with jax.named_scope("norm"):
        for r in range(4):
            tok_loads[r].wait()
            in_loads.append(load((w_q, w_k, w_v, w_p)[r], wts.at[r], w_sem.at[r]))

            @pl.loop(0, 8, unroll=4)
            def _(i):
                rows = pl.ds(pl.multiple_of(r * 128 + i * 16, 16), 16)
                wide = raw[rows].astype(F32)
                scale = lax.rsqrt(jnp.mean(wide * wide, axis=-1, keepdims=True) + EPS)
                normed[rows] = (wide * scale * gain[...]).astype(BF)

    def halves(i, finish_half):
        for r in range(2):
            rows = slice(256 * r, 256 * r + 256)
            finish_half(rows, jnp.dot(normed[rows], wts[i], preferred_element_type=F32))

    for cp in small[1:]:
        cp.wait()
    for hh in range(2):
        lam_in[hh] = jnp.full((8, 128), lam[hh], F32)
    with jax.named_scope("query"):
        in_loads[0].wait()

        def query_half(rows, value):
            value = value * (0.125 * LOG2E)
            for hh in range(2):
                q_in[hh, :, rows] = value[:, 128 * hh:128 * hh + 128].T.astype(BF)

        halves(0, query_half)
    pl.semaphore_wait(barrier, len(greeted))
    q_args = []
    for hh in range(2):
        q_args.append((q_in.at[hh], qraw.at[sq], q_send.at[hh], q_recv.at[sq], q_dst[hh]))
        q_args.append((lam_in.at[hh], lamb.at[sq], lam_send.at[hh], lam_recv.at[sq], q_dst[hh]))
    for a in q_args:
        send_any(*a)

    a2a_args = []
    for hh in range(2):
        for hf in range(2):
            a2a_args.append((kv_in.at[hh, hf], kv.at[z, hf, x], a2a_send.at[hh, hf], kv_recv.at[0, hf, x],
                             a2a_dst[hh][hf]))

    def hop_args(hh, hf):
        return (kv_in.at[hh, hf], x_relay, a2a_send.at[hh, hf], x_recv, dev(z, at(1 if hf == 0 else 3), hf))

    def exchange(hf):
        for hh in range(2):
            @pl.when(wrap(2 * c + hh - x) != 2)
            def _():
                send_any(*a2a_args[2 * hh + hf])

        for hh in range(2):
            @pl.when(wrap(2 * c + hh - x) == 2)
            def _():
                remote(*hop_args(hh, hf)).start()

    for i in range(1, 3):
        in_loads[i].wait()
    for hf in range(2):
        with jax.named_scope("keys_values"):
            rows = slice(256 * hf, 256 * hf + 256)
            keys = jnp.dot(normed[rows], wts[1], preferred_element_type=F32).astype(BF)
            values = jnp.dot(normed[rows], wts[2], preferred_element_type=F32)
            for hh in range(2):
                kv_in[hh, hf, 0:256] = keys[:, 128 * hh:128 * hh + 128]
                for j in range(2):
                    tile = values[128 * j:128 * j + 128, 128 * hh:128 * hh + 128]
                    kv_in[hh, hf, 256 + 128 * j:384 + 128 * j] = tile.T.astype(BF)
        exchange(hf)
    w_loads = [load(pool_proj, w_out.at[pl.ds(0, 256)], w_sem.at[4]),
               load(attn_proj, w_out.at[pl.ds(256, 256)], w_sem.at[5])]

    hop_from = jnp.where(c == 0, at(3), at(1))
    pass_args = (x_relay, kv.at[z, c, hop_from], pass_send, kv_recv.at[0, c, hop_from],
                 dev(z, jnp.where(c == 0, at(1), at(3)), c))


    def dd_args(rel, xk):
        piece = kv.at[wrap(z + rel), c, xk]
        return (piece, piece, dd_send.at[rel, xk], kv_recv.at[rel, c, xk], partner)

    def up_args(rel, xk):
        piece = kv.at[wrap(z + rel), c, xk]
        return (piece, piece, zp_send.at[rel & 1, xk], kv_recv.at[(rel + 3) % 4, c, xk], z_up)

    def dn_args(rel, xk):
        piece = kv.at[wrap(z + rel), c, xk]
        return (piece, piece, zm_send.at[rel & 1, xk], kv_recv.at[(rel + 1) % 4, c, xk], z_dn)

    def mine(rel, xk):
        arrived(kv.at[wrap(z + rel), c, xk], kv_recv.at[rel, c, xk])

    def go(args):
        remote(*args).start()

    mine(0, at(0))
    go(up_args(0, at(0)))
    go(dn_args(0, at(0)))
    go(dd_args(0, at(0)))

    with jax.named_scope("pool_in"):
        in_loads[3].wait()

        def pool_half(rows, value):
            pool_in[rows] = value.astype(BF)

        halves(3, pool_half)
    rim_args = (pool_in.at[pl.ds(ROWS - 16, 16)], rim, rim_send, rim_recv, nxt)
    remote(*rim_args).start()

    with jax.named_scope("own_near"):
        mine(0, at(1))
        go(up_args(0, at(1)))
        go(dd_args(0, at(1)))
        mine(0, at(3))
        go(dn_args(0, at(3)))
        go(up_args(0, at(3)))
        go(dd_args(0, at(3)))
        arrived(x_relay, x_recv)
        go(pass_args)

    with jax.named_scope("queries"):
        for s in range(2):
            arrived(qraw.at[s], q_recv.at[s])
            arrived(lamb.at[s], lam_recv.at[s])
            q = qraw[s]
            zero = jnp.zeros((64, ROWS), BF)
            qcat[s, 0] = jnp.concatenate([q[:64], zero], axis=0)
            qcat[s, 1] = jnp.concatenate([zero, q[64:]], axis=0)
            for m in range(2):
                top[s, m] = jnp.full((1, ROWS), NEG, F32)
                den[s, m] = jnp.zeros((1, ROWS), F32)
                acc[s, m] = jnp.zeros((128, ROWS), F32)

    def score(bank, zk, xk, s, m):
        keys = jnp.concatenate([kv[zk, hf, xk, 0:256] for hf in range(2)], axis=0)
        scores = jnp.dot(keys, qcat[s, m], preferred_element_type=F32)
        sbank[bank][...] = scores
        smax[bank] = jnp.max(scores, axis=0, keepdims=True)

    def weigh(bank, zk, xk, s, m, masked):
        vals = jnp.concatenate([kv[zk, hf, xk, 256 + 128 * j:384 + 128 * j] for hf in range(2) for j in range(2)],
                               axis=1)
        scores = sbank[bank][...]
        peak = smax[bank]
        if masked:
            allowed = (lax.div(lax.broadcasted_iota(jnp.int32, (ROWS, ROWS), 0), SEG)
                       <= lax.div(lax.broadcasted_iota(jnp.int32, (ROWS, ROWS), 1), SEG))
            scores = jnp.where(allowed, scores, NEG)
            peak = jnp.max(scores, axis=0, keepdims=True)
        old = top[s, m]
        new = jnp.maximum(old, peak)
        probs = jnp.exp2(scores - new)
        shrink = jnp.exp2(old - new)
        top[s, m] = new
        den[s, m] = den[s, m] * shrink + jnp.sum(probs, axis=0, keepdims=True)
        acc[s, m] = acc[s, m] * shrink + jnp.dot(vals, probs.astype(BF), preferred_element_type=F32)

    def attend(here, ahead, slots, masked):
        tiles = [(s, m) for s in slots for m in range(2)]
        for n, (s, m) in enumerate(tiles):
            if n + 1 < len(tiles):
                score((n + 1) % 2, *here, *tiles[n + 1])
            else:
                score(0, *ahead, 1, 0)
            weigh(n % 2, *here, s, m, masked == s)

    def joined(rel, xk):
        arrived(kv.at[wrap(z + rel), 1 - c, xk], kv_recv.at[rel, 1 - c, xk])

    def visit(here, ahead):
        block = here[0] * 4 + here[1]

        @pl.when(block <= qb[1])
        def _():
            @pl.when(block > qb[0])
            def _():
                @pl.when(block < qb[1])
                def _():
                    attend(here, ahead, (1,), None)

                @pl.when(block == qb[1])
                def _():
                    attend(here, ahead, (1,), 1)

            @pl.when(block <= qb[0])
            def _():
                @pl.when(block < qb[0])
                def _():
                    attend(here, ahead, (1, 0), None)

                @pl.when(block == qb[0])
                def _():
                    attend(here, ahead, (1, 0), 0)

        @pl.when(block > qb[1])
        def _():
            score(0, *ahead, 1, 0)

    below, above = (0, 1, 3, 2), (0, 3, 2, 1)
    plan = ([(0, o) for o in below] + [p for i in range(4) for p in ((3, below[i]), (1, above[i]))]
            + [(2, o) for o in (0, 3, 1, 2)])

    def near(i):
        mine(3, at(below[i]))
        if i < 2:
            go(up_args(3, at(below[i])))
        go(dd_args(3, at(below[i])))
        mine(1, at(above[i]))
        if i in (1, 2):
            go(dn_args(1, at(above[i])))
        go(dd_args(1, at(above[i])))

    def far(i):
        for off in ((0, 3), (1, 2))[i]:
            mine(2, at(off))
            go(dd_args(2, at(off)))

    def pooling(_):
        arrived(rim, rim_recv)
        edge = jnp.where(sp == 0, 0.0, rim[...].astype(F32))
        own = pool_in[...].astype(F32)
        lane = lax.broadcasted_iota(jnp.int32, (1, 128), 1)
        totals = []
        for side in range(2):
            cols = slice(128 * side, 128 * side + 128)
            line = jnp.concatenate([edge[:, cols], own[:, cols]], axis=0)
            s2 = line + pltpu.roll(line, 1, 0)
            s4 = s2 + pltpu.roll(s2, 2, 0)
            if side == 0:
                totals.append(jnp.where(lane < 64, s2, s4)[16:])
            else:
                s8 = s4 + pltpu.roll(s4, 4, 0)
                s16 = s8 + pltpu.roll(s8, 8, 0)
                totals.append(jnp.where(lane < 64, s8, s16)[16:])
        total = jnp.concatenate(totals, axis=1)
        lane = lax.broadcasted_iota(jnp.int32, (1, 256), 1)
        window = jnp.where(lane < 64, 2, jnp.where(lane < 128, 4, jnp.where(lane < 192, 8, 16)))
        position = sp * ROWS + lax.broadcasted_iota(jnp.int32, (16, 256), 0)
        early = total[:16] / jnp.minimum(position + 1, window).astype(F32)
        later = total[16:] * (1.0 / window.astype(F32))
        mixed_in = (jnp.concatenate([early, later], axis=0) - own).astype(BF)
        spread = (lax.rem(lax.broadcasted_iota(jnp.int32, (64, 256), 1), 64)
                  == lax.broadcasted_iota(jnp.int32, (64, 256), 0)).astype(F32).astype(BF)
        wide_mix = jnp.dot(pool_mix[...], spread, preferred_element_type=F32)
        same = (lax.div(lax.broadcasted_iota(jnp.int32, (256, 256), 0), 64)
                == lax.div(lax.broadcasted_iota(jnp.int32, (256, 256), 1), 64))
        block_mix = jnp.where(same, wide_mix, 0.0).astype(BF)
        grouped = jnp.dot(mixed_in, block_mix, preferred_element_type=F32)
        pooled[...] = (grouped * pool_scale[...]).astype(BF)

    def own_far(_):
        mine(0, at(2))
        go(dn_args(0, at(2)))
        go(up_args(0, at(2)))
        go(dd_args(0, at(2)))
        go(dn_args(0, at(1)))

    service = {0: (near, 0), 2: (own_far, 0), 3: (near, 1), 5: (near, 2), 7: (near, 3), 9: (pooling, 0), 10: (far, 0),
               12: (far, 1)}

    mine_h = lax.rem(x, 2)
    ret_args = [(ao.at[s], ab.at[mine_h], ret_send.at[s], ret_recv.at[mine_h], q_src[s]) for s in range(2)]

    def finish(s):
        o1 = acc[s, 0] / den[s, 0]
        o2 = acc[s, 1] / den[s, 1]
        blend = o1 - lamb[s][0:1, 0:1] * o2
        scaled = blend * lax.rsqrt(jnp.mean(blend * blend, axis=0, keepdims=True) + EPS)
        ao[s] = (scaled.T * head_gain[...] * 0.8).astype(BF)
        send_any(*ret_args[s])

    soon = wrap(z + 2) * 4 > qb[0]

    with jax.named_scope("attend"):
        joined(0, at(0))
        score(0, z, at(0), 1, 0)

        @pl.loop(0, 16)
        def _(v):
            @pl.when(pick(v, [int(i in service) for i in range(16)]) == 1)
            def _():
                for when, (serve, i) in service.items():
                    @pl.when(v == when)
                    def _():
                        with jax.named_scope(f"serve{when}"):
                            serve(i)

            @pl.when((v == 12) & soon)
            def _():
                finish(0)

            follow = jnp.minimum(v + 1, 15)
            rel, nrel = (pick(i, [p[0] for p in plan]) for i in (v, follow))
            xk, nxk = (at(pick(i, [p[1] for p in plan])) for i in (v, follow))

            @pl.when(v < 15)
            def _():
                with jax.named_scope("join"):
                    joined(nrel, nxk)

            with jax.named_scope("visit"):
                visit((wrap(z + rel), xk), (wrap(z + nrel), nxk))

    with jax.named_scope("finish"):
        finish(1)

        @pl.when(jnp.logical_not(soon))
        def _():
            finish(0)

    with jax.named_scope("drain"):
        remote(*rim_args).wait_send()
        for a in a2a_args + q_args:
            sent_any(*a)
        remote(*pass_args).wait_send()
        for off in range(4):
            remote(*up_args(0, at(off))).wait_send()
            remote(*dn_args(0, at(off))).wait_send()
            for rel in range(4):
                remote(*dd_args(rel, at(off))).wait_send()
        for i in range(2):
            remote(*up_args(3, at(below[i]))).wait_send()
            remote(*dn_args(1, at(above[i + 1]))).wait_send()

    for cp in w_loads:
        cp.wait()
    with jax.named_scope("home"):
        for hh in range(2):
            arrived(ab.at[hh], ret_recv.at[hh])

    order = [wrap(y + 2), wrap(y + 1), wrap(y - 1), y]

    def pd_args(h, k):
        return (pbuf.at[h, 2 * order[k] + 1 - c], dbuf.at[h, k], pd_send.at[h, k], pd_recv.at[h, k], partner)

    def project(h):
        feats = jnp.concatenate([pooled[...], ab[0], ab[1]], axis=1)
        term = jnp.dot(feats, w_out[:, 1024 * h:1024 * h + 1024], preferred_element_type=F32)
        pbuf[h] = term.astype(BF).reshape(8, 64, 1024)
        for k in range(4):
            go(pd_args(h, k))

    def chip_sum(h, k):
        arrived(dbuf.at[h, k], pd_recv.at[h, k])
        return pbuf[h, 2 * order[k] + c].astype(F32) + dbuf[h, k].astype(F32)

    def relay_args(h):
        return (sbuf.at[0, h], relay.at[h], y_send.at[0, h], y_recv.at[0, h], y_up if h < 2 else y_dn)

    def up_sum_args(h):
        return (sbuf.at[1, h], fin.at[0, h], y_send.at[1, h], y_recv.at[1, h], y_up)

    def dn_sum_args(h):
        return (sbuf.at[2, h], fin.at[1, h], y_send.at[2, h], y_recv.at[2, h], y_dn)

    def put(i, h, value, args):
        sbuf[i, h] = value.astype(BF)
        go(args)

    def start_relay(h):
        put(0, h, chip_sum(h, 0), relay_args(h))

    def direct(h):
        if h < 2:
            put(2, h, chip_sum(h, 2), dn_sum_args(h))
        else:
            put(1, h, chip_sum(h, 1), up_sum_args(h))

    def relayed(h):
        own_sum = chip_sum(h, 1 if h < 2 else 2)
        arrived(relay.at[h], y_recv.at[0, h])
        value = own_sum + relay[h].astype(F32)
        if h < 2:
            put(1, h, value, up_sum_args(h))
        else:
            put(2, h, value, dn_sum_args(h))

    with jax.named_scope("out_first"):
        project(0)
        project(2)
        start_relay(0)
        start_relay(2)
        direct(0)
        direct(2)
    with jax.named_scope("out_second"):
        project(1)
        project(3)
        start_relay(1)
        start_relay(3)
        direct(1)
        direct(3)
    with jax.named_scope("out_relayed"):
        for h in (0, 2, 1, 3):
            relayed(h)
    stores = []
    with jax.named_scope("out_last"):
        for h in (2, 0, 3, 1):
            own_sum = chip_sum(h, 3)
            arrived(fin.at[0, h], y_recv.at[1, h])
            arrived(fin.at[1, h], y_recv.at[2, h])
            whole = own_sum + fin[0, h].astype(F32) + fin[1, h].astype(F32)
            cols = pl.ds(1024 * h, 1024)
            out_buf[:, cols] = whole.astype(BF)
            stores.append(load(out_buf.at[:, cols], out.at[:, cols], out_sem.at[h]))

    for a in ret_args:
        sent_any(*a)
    for cp in stores:
        cp.wait()
    for h in range(4):
        for k in range(4):
            remote(*pd_args(h, k)).wait_send()
        remote(*relay_args(h)).wait_send()
        remote(*up_sum_args(h)).wait_send()
        remote(*dn_sum_args(h)).wait_send()


def body(tokens, norm_gain, w_pool_in, w_query, w_key, w_value, pool_mix, pool_scale, lam, head_gain,
         pool_proj, attn_proj):
    sd = jax.ShapeDtypeStruct
    dma = pltpu.SemaphoreType.DMA
    return pl.pallas_call(
        mixer_kernel,
        out_shape=sd((64, WIDE), BF),
        in_specs=[ANY] * 12,
        out_specs=ANY,
        scratch_shapes=[
            pltpu.VMEM((1, WIDE), F32),
            pltpu.SMEM((2,), F32),
            pltpu.VMEM((256, 64), BF),
            pltpu.VMEM((1, 256), F32),
            pltpu.VMEM((1, 128), F32),
            pltpu.VMEM((64, WIDE), BF),
            dma((5,)), dma((4,)),
            pltpu.VMEM((ROWS, WIDE), BF),
            pltpu.VMEM((ROWS, WIDE), BF),
            pltpu.VMEM((4, WIDE, 256), BF),
            pltpu.VMEM((2, 2, 512, 128), BF),
            pltpu.VMEM((2, 128, ROWS), BF),
            pltpu.VMEM((ROWS, 256), BF),
            pltpu.VMEM((2, 8, 128), F32),
            pltpu.VMEM((4, 2, 4, 512, 128), BF),
            pltpu.VMEM((2, 128, ROWS), BF),
            pltpu.VMEM((2, 2, 128, ROWS), BF),
            pltpu.VMEM((2, 8, 128), F32),
            pltpu.VMEM((16, 256), BF),
            pltpu.VMEM((2, 2, 128, ROWS), F32),
            pltpu.VMEM((2, 2, 1, ROWS), F32),
            pltpu.VMEM((2, 2, 1, ROWS), F32),
            pltpu.VMEM((ROWS, ROWS), F32),
            pltpu.VMEM((ROWS, ROWS), F32),
            pltpu.VMEM((2, 1, ROWS), F32),
            pltpu.VMEM((512, 128), BF),
            pltpu.VMEM((2, ROWS, 128), BF),
            pltpu.VMEM((2, ROWS, 128), BF),
            pltpu.VMEM((ROWS, 256), BF),
            pltpu.VMEM((512, WIDE), BF),
            pltpu.VMEM((4, 8, 64, 1024), BF),
            pltpu.VMEM((4, 4, 64, 1024), BF),
            pltpu.VMEM((3, 4, 64, 1024), BF),
            pltpu.VMEM((4, 64, 1024), BF),
            pltpu.VMEM((2, 4, 64, 1024), BF),
            dma((4,)), dma((6,)), dma, dma, dma((2, 2)), dma((4, 2, 4)), dma((2,)), dma((2,)), dma((2,)), dma((2,)),
            dma, dma, dma((2, 4)), dma((2, 4)), dma((4, 4)), dma((2,)), dma((2,)),
            dma((4, 4)), dma((4, 4)), dma((3, 4)), dma((3, 4)),
        ],
        compiler_params=pltpu.CompilerParams(vmem_limit_bytes=67043328, collective_id=0, has_side_effects=True),
        name="mixer",
    )(tokens, norm_gain.reshape(1, WIDE), w_key, w_value, w_query, w_pool_in, lam, pool_mix.reshape(256, 64),
      pool_scale.reshape(1, 256), head_gain.reshape(1, 128), pool_proj, attn_proj)


def solution(mesh):
    return jax.shard_map(
        body,
        mesh=mesh,
        in_specs=(P("sp", None), P(), P(None, "tp"), P(None, "tp"), P(None, "tp"), P(None, "tp"),
                  P("tp", None, None), P("tp"), P("tp"), P(), P("tp", None), P("tp", None)),
        out_specs=P(("sp", "tp"), None),
        check_vma=False,
    )
```

```python
import jax
import jax.numpy as jnp
from jax import lax
from jax.experimental import pallas as pl
from jax.experimental.pallas import tpu as pltpu
from jax.sharding import PartitionSpec as P

EPS = 1e-6
NEG = -1e30
LOG2E = 1.4426950408889634
ROWS = 512
WIDE = 4096
SEG = 64
BF = jnp.bfloat16
F32 = jnp.float32
MESH_ID = pl.DeviceIdType.MESH
OUTER = ((2, 3, 0, 1), (0, 3, 1, 2), (3, 2, 1, 0), (1, 0, 3, 2))
INNER = ((0, 2, 1, 3), (2, 1, 3, 0), (1, 0, 3, 2), (3, 2, 1, 0))


def pick(at, values):
    packed = sum(value << (2 * i) for i, value in enumerate(values))
    packed = packed - (1 << 32) if packed >= 1 << 31 else packed
    return lax.shift_right_logical(jnp.int32(packed), 2 * at) & 3


def flat(table):
    return [value for row in table for value in row]


def inverse(table):
    return [row.index(value) for row in table for value in range(4)]
ANY = pl.BlockSpec(memory_space=pl.ANY)


def mixer_kernel(tok, gain_in, w_k, w_v, w_q, w_p, lam_hbm, mix_in, scale_in, head_gain_in, pool_proj, attn_proj,
                 out,
                 gain, lam, pool_mix, pool_scale, head_gain, out_buf, small_sem, out_sem, raw, normed, wts, kv_in, q_in, pool_in, lam_in, kv, qraw, qcat, lamb, rim, acc, top, den, sbank_a, sbank_b, smax, x_relay, ao, ab, pooled, w_out, pbuf, dbuf, sbuf, relay, fin,
                 tok_sem, w_sem, x_recv, pass_send, a2a_send, kv_recv, q_send, q_recv, lam_send, lam_recv, rim_send, rim_recv,
                 zp_send, zm_send, dd_send, ret_send, ret_recv, pd_send, pd_recv, y_send, y_recv):
    sbank = (sbank_a, sbank_b)
    sp = lax.axis_index("sp")
    tp = lax.axis_index("tp")
    z, x = lax.shift_right_logical(sp, 2), sp & 3
    y, c = lax.shift_right_logical(tp, 1), tp & 1

    def wrap(i):
        return (i + 4) & 3

    def dev(zz, xx, cc):
        return (zz * 4 + xx, y * 2 + cc)

    def at(off):
        return (x + off) & 3

    me = (sp, tp)

    def is_me(d):
        return (d[0] == sp) & (d[1] == tp)

    core_src = lax.div(x, 2)
    outer_row = (z == 0) | (z == 3)
    place = jnp.where(z < 2, x, 3 - x)
    cq = jnp.where(outer_row, 0, 1)
    sq = lax.div(z, 2)
    a_here, b_here = pick(x * 4 + z, flat(OUTER)), pick(x * 4 + z, flat(INNER))
    qb = [jnp.where(c == 0, a_here, 4 + b_here), jnp.where(c == 0, 15 - a_here, 11 - b_here)]
    partner = dev(z, x, 1 - c)
    z_up, z_dn = dev(wrap(z + 1), x, c), dev(wrap(z - 1), x, c)
    y_up = (sp, wrap(y + 1) * 2 + c)
    y_dn = (sp, wrap(y - 1) * 2 + c)
    nxt = (lax.rem(sp + 1, 16), tp)
    prv = (lax.rem(sp + 15, 16), tp)
    a2a_dst = [[dev(z, 2 * c + hh, hf) for hf in range(2)] for hh in range(2)]
    q_dst = []
    for hh in range(2):
        spot = (2 * c + hh) * 4 + place
        q_dst.append(dev(jnp.where(outer_row, pick(spot, inverse(OUTER)), pick(spot, inverse(INNER))), 2 * c + hh, cq))
    q_src = [dev(lax.div(qb[s], 4), lax.rem(qb[s], 4), core_src) for s in range(2)]

    def load(src, dst, sem):
        cp = pltpu.make_async_copy(src, dst, sem)
        cp.start()
        return cp

    tok_loads = [load(tok.at[pl.ds(r * 128, 128)], raw.at[pl.ds(r * 128, 128)], tok_sem.at[r]) for r in range(4)]
    small = [load(src, dst, small_sem.at[i]) for i, (src, dst) in enumerate(
        ((gain_in, gain), (lam_hbm, lam), (mix_in, pool_mix), (scale_in, pool_scale), (head_gain_in, head_gain)))]
    in_loads = []

    barrier = pltpu.get_barrier_semaphore()

    def greet(d):
        pl.semaphore_signal(barrier, inc=1, device_id=d, device_id_type=MESH_ID)

    behind, beyond = jnp.where(c == 0, at(3), at(1)), jnp.where(c == 0, at(1), at(3))
    greeted = [dev(z, at(off), core_src) for off in (0, 1, 3)] + [dev(z, behind, lax.div(beyond, 2)), dev(z, behind, c)]
    greeted = greeted + q_src + q_dst + [z_up, z_dn, partner, y_up, y_dn, prv]
    for d in greeted:
        greet(d)

    def remote(src, dst, ssem, rsem, d):
        return pltpu.make_async_remote_copy(src_ref=src, dst_ref=dst, send_sem=ssem, recv_sem=rsem,
                                            device_id=d, device_id_type=MESH_ID)

    def send_any(src, dst, ssem, rsem, d):
        @pl.when(is_me(d))
        def _():
            pltpu.make_async_copy(src, dst, rsem).start()

        @pl.when(jnp.logical_not(is_me(d)))
        def _():
            remote(src, dst, ssem, rsem, d).start()

    def sent_any(src, dst, ssem, rsem, d):
        @pl.when(jnp.logical_not(is_me(d)))
        def _():
            remote(src, dst, ssem, rsem, d).wait_send()

    def arrived(dst, rsem):
        pltpu.make_async_copy(dst, dst, rsem).wait()

    small[0].wait()
    with jax.named_scope("norm"):
        for r in range(4):
            tok_loads[r].wait()
            in_loads.append(load((w_q, w_k, w_v, w_p)[r], wts.at[r], w_sem.at[r]))

            @pl.loop(0, 8, unroll=4)
            def _(i):
                rows = pl.ds(pl.multiple_of(r * 128 + i * 16, 16), 16)
                wide = raw[rows].astype(F32)
                scale = lax.rsqrt(jnp.mean(wide * wide, axis=-1, keepdims=True) + EPS)
                normed[rows] = (wide * scale * gain[...]).astype(BF)

    def halves(i, finish_half):
        for r in range(2):
            rows = slice(256 * r, 256 * r + 256)
            finish_half(rows, jnp.dot(normed[rows], wts[i], preferred_element_type=F32))

    for cp in small[1:]:
        cp.wait()
    for hh in range(2):
        lam_in[hh] = jnp.full((8, 128), lam[hh], F32)
    with jax.named_scope("query"):
        in_loads[0].wait()

        def query_half(rows, value):
            value = value * (0.125 * LOG2E)
            for hh in range(2):
                q_in[hh, :, rows] = value[:, 128 * hh:128 * hh + 128].T.astype(BF)

        halves(0, query_half)
    pl.semaphore_wait(barrier, len(greeted))
    q_args = []
    for hh in range(2):
        q_args.append((q_in.at[hh], qraw.at[sq], q_send.at[hh], q_recv.at[sq], q_dst[hh]))
        q_args.append((lam_in.at[hh], lamb.at[sq], lam_send.at[hh], lam_recv.at[sq], q_dst[hh]))
    for a in q_args:
        send_any(*a)

    a2a_args = []
    for hh in range(2):
        for hf in range(2):
            a2a_args.append((kv_in.at[hh, hf], kv.at[z, hf, x], a2a_send.at[hh, hf], kv_recv.at[0, hf, x],
                             a2a_dst[hh][hf]))

    def hop_args(hh, hf):
        return (kv_in.at[hh, hf], x_relay, a2a_send.at[hh, hf], x_recv, dev(z, at(1 if hf == 0 else 3), hf))

    def exchange(hf):
        for hh in range(2):
            @pl.when(wrap(2 * c + hh - x) != 2)
            def _():
                send_any(*a2a_args[2 * hh + hf])

    def exchange_far(hf):
        for hh in range(2):
            @pl.when(wrap(2 * c + hh - x) == 2)
            def _():
                remote(*hop_args(hh, hf)).start()

    for i in range(1, 3):
        in_loads[i].wait()
    for hf in range(2):
        with jax.named_scope("keys_values"):
            rows = slice(256 * hf, 256 * hf + 256)
            keys = jnp.dot(normed[rows], wts[1], preferred_element_type=F32).astype(BF)
            values = jnp.dot(normed[rows], wts[2], preferred_element_type=F32)
            for hh in range(2):
                kv_in[hh, hf, 0:256] = keys[:, 128 * hh:128 * hh + 128]
                for j in range(2):
                    tile = values[128 * j:128 * j + 128, 128 * hh:128 * hh + 128]
                    kv_in[hh, hf, 256 + 128 * j:384 + 128 * j] = tile.T.astype(BF)
        exchange(hf)
    w_loads = [load(pool_proj, w_out.at[pl.ds(0, 256)], w_sem.at[4]),
               load(attn_proj, w_out.at[pl.ds(256, 256)], w_sem.at[5])]

    hop_from = jnp.where(c == 0, at(3), at(1))
    pass_args = (x_relay, kv.at[z, c, hop_from], pass_send, kv_recv.at[0, c, hop_from],
                 dev(z, jnp.where(c == 0, at(1), at(3)), c))


    def dd_args(rel, xk):
        piece = kv.at[wrap(z + rel), c, xk]
        return (piece, piece, dd_send.at[rel, xk], kv_recv.at[rel, c, xk], partner)

    def up_args(rel, xk):
        piece = kv.at[wrap(z + rel), c, xk]
        return (piece, piece, zp_send.at[rel & 1, xk], kv_recv.at[(rel + 3) % 4, c, xk], z_up)

    def dn_args(rel, xk):
        piece = kv.at[wrap(z + rel), c, xk]
        return (piece, piece, zm_send.at[rel & 1, xk], kv_recv.at[(rel + 1) % 4, c, xk], z_dn)

    def mine(rel, xk):
        arrived(kv.at[wrap(z + rel), c, xk], kv_recv.at[rel, c, xk])

    def go(args):
        remote(*args).start()

    mine(0, at(0))
    go(up_args(0, at(0)))
    go(dn_args(0, at(0)))
    go(dd_args(0, at(0)))

    with jax.named_scope("pool_in"):
        in_loads[3].wait()

        def pool_half(rows, value):
            pool_in[rows] = value.astype(BF)

        halves(3, pool_half)
    rim_args = (pool_in.at[pl.ds(ROWS - 16, 16)], rim, rim_send, rim_recv, nxt)
    remote(*rim_args).start()
    for hf in range(2):
        exchange_far(hf)

    with jax.named_scope("own_near"):
        mine(0, at(1))
        go(up_args(0, at(1)))
        go(dd_args(0, at(1)))
        mine(0, at(3))
        go(dn_args(0, at(3)))
        go(up_args(0, at(3)))
        go(dd_args(0, at(3)))
        arrived(x_relay, x_recv)
        go(pass_args)

    with jax.named_scope("queries"):
        for s in range(2):
            arrived(qraw.at[s], q_recv.at[s])
            arrived(lamb.at[s], lam_recv.at[s])
            q = qraw[s]
            zero = jnp.zeros((64, ROWS), BF)
            qcat[s, 0] = jnp.concatenate([q[:64], zero], axis=0)
            qcat[s, 1] = jnp.concatenate([zero, q[64:]], axis=0)
            for m in range(2):
                top[s, m] = jnp.full((1, ROWS), NEG, F32)
                den[s, m] = jnp.zeros((1, ROWS), F32)
                acc[s, m] = jnp.zeros((128, ROWS), F32)

    def score(bank, zk, xk, s, m):
        keys = jnp.concatenate([kv[zk, hf, xk, 0:256] for hf in range(2)], axis=0)
        scores = jnp.dot(keys, qcat[s, m], preferred_element_type=F32)
        sbank[bank][...] = scores
        smax[bank] = jnp.max(scores, axis=0, keepdims=True)

    def weigh(bank, zk, xk, s, m, masked):
        vals = jnp.concatenate([kv[zk, hf, xk, 256 + 128 * j:384 + 128 * j] for hf in range(2) for j in range(2)],
                               axis=1)
        scores = sbank[bank][...]
        peak = smax[bank]
        if masked:
            allowed = (lax.div(lax.broadcasted_iota(jnp.int32, (ROWS, ROWS), 0), SEG)
                       <= lax.div(lax.broadcasted_iota(jnp.int32, (ROWS, ROWS), 1), SEG))
            scores = jnp.where(allowed, scores, NEG)
            peak = jnp.max(scores, axis=0, keepdims=True)
        old = top[s, m]
        new = jnp.maximum(old, peak)
        probs = jnp.exp2(scores - new)
        shrink = jnp.exp2(old - new)
        top[s, m] = new
        den[s, m] = den[s, m] * shrink + jnp.sum(probs, axis=0, keepdims=True)
        acc[s, m] = acc[s, m] * shrink + jnp.dot(vals, probs.astype(BF), preferred_element_type=F32)

    def attend(here, ahead, slots, masked):
        tiles = [(s, m) for s in slots for m in range(2)]
        for n, (s, m) in enumerate(tiles):
            if n + 1 < len(tiles):
                score((n + 1) % 2, *here, *tiles[n + 1])
            else:
                score(0, *ahead, 1, 0)
            weigh(n % 2, *here, s, m, masked == s)

    def joined(rel, xk):
        arrived(kv.at[wrap(z + rel), 1 - c, xk], kv_recv.at[rel, 1 - c, xk])

    def visit(here, ahead):
        block = here[0] * 4 + here[1]

        @pl.when(block <= qb[1])
        def _():
            @pl.when(block > qb[0])
            def _():
                @pl.when(block < qb[1])
                def _():
                    attend(here, ahead, (1,), None)

                @pl.when(block == qb[1])
                def _():
                    attend(here, ahead, (1,), 1)

            @pl.when(block <= qb[0])
            def _():
                @pl.when(block < qb[0])
                def _():
                    attend(here, ahead, (1, 0), None)

                @pl.when(block == qb[0])
                def _():
                    attend(here, ahead, (1, 0), 0)

        @pl.when(block > qb[1])
        def _():
            score(0, *ahead, 1, 0)

    below, above = (0, 1, 3, 2), (0, 3, 2, 1)
    plan = [(0, 0), (0, 1), (0, 3), (3, 0), (1, 0), (0, 2), (3, 1), (1, 3), (3, 3), (1, 2), (3, 2), (1, 1),
            (2, 0), (2, 3), (2, 1), (2, 2)]

    def near(i):
        mine(3, at(below[i]))
        if i < 2:
            go(up_args(3, at(below[i])))
        go(dd_args(3, at(below[i])))
        mine(1, at(above[i]))
        if i in (1, 2):
            go(dn_args(1, at(above[i])))
        go(dd_args(1, at(above[i])))

    def far(i):
        for off in ((0, 3), (1, 2))[i]:
            mine(2, at(off))
            go(dd_args(2, at(off)))

    def pooling(_):
        arrived(rim, rim_recv)
        edge = jnp.where(sp == 0, 0.0, rim[...].astype(F32))
        own = pool_in[...].astype(F32)
        lane = lax.broadcasted_iota(jnp.int32, (1, 128), 1)
        totals = []
        for side in range(2):
            cols = slice(128 * side, 128 * side + 128)
            line = jnp.concatenate([edge[:, cols], own[:, cols]], axis=0)
            s2 = line + pltpu.roll(line, 1, 0)
            s4 = s2 + pltpu.roll(s2, 2, 0)
            if side == 0:
                totals.append(jnp.where(lane < 64, s2, s4)[16:])
            else:
                s8 = s4 + pltpu.roll(s4, 4, 0)
                s16 = s8 + pltpu.roll(s8, 8, 0)
                totals.append(jnp.where(lane < 64, s8, s16)[16:])
        total = jnp.concatenate(totals, axis=1)
        lane = lax.broadcasted_iota(jnp.int32, (1, 256), 1)
        window = jnp.where(lane < 64, 2, jnp.where(lane < 128, 4, jnp.where(lane < 192, 8, 16)))
        position = sp * ROWS + lax.broadcasted_iota(jnp.int32, (16, 256), 0)
        early = total[:16] / jnp.minimum(position + 1, window).astype(F32)
        later = total[16:] * (1.0 / window.astype(F32))
        mixed_in = (jnp.concatenate([early, later], axis=0) - own).astype(BF)
        spread = (lax.rem(lax.broadcasted_iota(jnp.int32, (64, 256), 1), 64)
                  == lax.broadcasted_iota(jnp.int32, (64, 256), 0)).astype(F32).astype(BF)
        wide_mix = jnp.dot(pool_mix[...], spread, preferred_element_type=F32)
        same = (lax.div(lax.broadcasted_iota(jnp.int32, (256, 256), 0), 64)
                == lax.div(lax.broadcasted_iota(jnp.int32, (256, 256), 1), 64))
        block_mix = jnp.where(same, wide_mix, 0.0).astype(BF)
        grouped = jnp.dot(mixed_in, block_mix, preferred_element_type=F32)
        pooled[...] = (grouped * pool_scale[...]).astype(BF)

    def own_far(_):
        mine(0, at(2))
        go(dn_args(0, at(2)))
        go(up_args(0, at(2)))
        go(dd_args(0, at(2)))
        go(dn_args(0, at(1)))

    service = {1: (near, 0), 3: (own_far, 0), 5: (near, 1), 7: (near, 2), 8: (near, 3), 9: (pooling, 0), 10: (far, 0),
               12: (far, 1)}

    mine_h = lax.rem(x, 2)
    ret_args = [(ao.at[s], ab.at[mine_h], ret_send.at[s], ret_recv.at[mine_h], q_src[s]) for s in range(2)]

    def finish(s):
        o1 = acc[s, 0] / den[s, 0]
        o2 = acc[s, 1] / den[s, 1]
        blend = o1 - lamb[s][0:1, 0:1] * o2
        scaled = blend * lax.rsqrt(jnp.mean(blend * blend, axis=0, keepdims=True) + EPS)
        ao[s] = (scaled.T * head_gain[...] * 0.8).astype(BF)
        send_any(*ret_args[s])

    soon = wrap(z + 2) * 4 > qb[0]

    with jax.named_scope("attend"):
        joined(0, at(0))
        score(0, z, at(0), 1, 0)

        @pl.loop(0, 16)
        def _(v):
            @pl.when(pick(v, [int(i in service) for i in range(16)]) == 1)
            def _():
                for when, (serve, i) in service.items():
                    @pl.when(v == when)
                    def _():
                        with jax.named_scope(f"serve{when}"):
                            serve(i)

            @pl.when((v == 12) & soon)
            def _():
                finish(0)

            follow = jnp.minimum(v + 1, 15)
            rel, nrel = (pick(i, [p[0] for p in plan]) for i in (v, follow))
            xk, nxk = (at(pick(i, [p[1] for p in plan])) for i in (v, follow))

            @pl.when(v < 15)
            def _():
                with jax.named_scope("join"):
                    joined(nrel, nxk)

            with jax.named_scope("visit"):
                visit((wrap(z + rel), xk), (wrap(z + nrel), nxk))

    with jax.named_scope("finish"):
        finish(1)

        @pl.when(jnp.logical_not(soon))
        def _():
            finish(0)

    with jax.named_scope("drain"):
        remote(*rim_args).wait_send()
        for a in a2a_args + q_args:
            sent_any(*a)
        remote(*pass_args).wait_send()
        for off in range(4):
            remote(*up_args(0, at(off))).wait_send()
            remote(*dn_args(0, at(off))).wait_send()
            for rel in range(4):
                remote(*dd_args(rel, at(off))).wait_send()
        for i in range(2):
            remote(*up_args(3, at(below[i]))).wait_send()
            remote(*dn_args(1, at(above[i + 1]))).wait_send()

    for cp in w_loads:
        cp.wait()
    with jax.named_scope("home"):
        for hh in range(2):
            arrived(ab.at[hh], ret_recv.at[hh])

    order = [wrap(y + 2), wrap(y + 1), wrap(y - 1), y]

    def pd_args(h, k):
        return (pbuf.at[h, 2 * order[k] + 1 - c], dbuf.at[h, k], pd_send.at[h, k], pd_recv.at[h, k], partner)

    def project(h):
        feats = jnp.concatenate([pooled[...], ab[0], ab[1]], axis=1)
        term = jnp.dot(feats, w_out[:, 1024 * h:1024 * h + 1024], preferred_element_type=F32)
        pbuf[h] = term.astype(BF).reshape(8, 64, 1024)
        for k in range(4):
            go(pd_args(h, k))

    def chip_sum(h, k):
        arrived(dbuf.at[h, k], pd_recv.at[h, k])
        return pbuf[h, 2 * order[k] + c].astype(F32) + dbuf[h, k].astype(F32)

    def relay_args(h):
        return (sbuf.at[0, h], relay.at[h], y_send.at[0, h], y_recv.at[0, h], y_up if h < 2 else y_dn)

    def up_sum_args(h):
        return (sbuf.at[1, h], fin.at[0, h], y_send.at[1, h], y_recv.at[1, h], y_up)

    def dn_sum_args(h):
        return (sbuf.at[2, h], fin.at[1, h], y_send.at[2, h], y_recv.at[2, h], y_dn)

    def put(i, h, value, args):
        sbuf[i, h] = value.astype(BF)
        go(args)

    def start_relay(h):
        put(0, h, chip_sum(h, 0), relay_args(h))

    def direct(h):
        if h < 2:
            put(2, h, chip_sum(h, 2), dn_sum_args(h))
        else:
            put(1, h, chip_sum(h, 1), up_sum_args(h))

    def relayed(h):
        own_sum = chip_sum(h, 1 if h < 2 else 2)
        arrived(relay.at[h], y_recv.at[0, h])
        value = own_sum + relay[h].astype(F32)
        if h < 2:
            put(1, h, value, up_sum_args(h))
        else:
            put(2, h, value, dn_sum_args(h))

    with jax.named_scope("out_first"):
        project(0)
        project(2)
        start_relay(0)
        start_relay(2)
        direct(0)
        direct(2)
    with jax.named_scope("out_second"):
        project(1)
        project(3)
        start_relay(1)
        start_relay(3)
        direct(1)
        direct(3)
    with jax.named_scope("out_relayed"):
        for h in (0, 2, 1, 3):
            relayed(h)
    stores = []
    with jax.named_scope("out_last"):
        for h in (2, 0, 3, 1):
            own_sum = chip_sum(h, 3)
            arrived(fin.at[0, h], y_recv.at[1, h])
            arrived(fin.at[1, h], y_recv.at[2, h])
            whole = own_sum + fin[0, h].astype(F32) + fin[1, h].astype(F32)
            cols = pl.ds(1024 * h, 1024)
            out_buf[:, cols] = whole.astype(BF)
            stores.append(load(out_buf.at[:, cols], out.at[:, cols], out_sem.at[h]))

    for a in ret_args:
        sent_any(*a)
    for cp in stores:
        cp.wait()
    for h in range(4):
        for k in range(4):
            remote(*pd_args(h, k)).wait_send()
        remote(*relay_args(h)).wait_send()
        remote(*up_sum_args(h)).wait_send()
        remote(*dn_sum_args(h)).wait_send()


def body(tokens, norm_gain, w_pool_in, w_query, w_key, w_value, pool_mix, pool_scale, lam, head_gain,
         pool_proj, attn_proj):
    sd = jax.ShapeDtypeStruct
    dma = pltpu.SemaphoreType.DMA
    return pl.pallas_call(
        mixer_kernel,
        out_shape=sd((64, WIDE), BF),
        in_specs=[ANY] * 12,
        out_specs=ANY,
        scratch_shapes=[
            pltpu.VMEM((1, WIDE), F32),
            pltpu.SMEM((2,), F32),
            pltpu.VMEM((256, 64), BF),
            pltpu.VMEM((1, 256), F32),
            pltpu.VMEM((1, 128), F32),
            pltpu.VMEM((64, WIDE), BF),
            dma((5,)), dma((4,)),
            pltpu.VMEM((ROWS, WIDE), BF),
            pltpu.VMEM((ROWS, WIDE), BF),
            pltpu.VMEM((4, WIDE, 256), BF),
            pltpu.VMEM((2, 2, 512, 128), BF),
            pltpu.VMEM((2, 128, ROWS), BF),
            pltpu.VMEM((ROWS, 256), BF),
            pltpu.VMEM((2, 8, 128), F32),
            pltpu.VMEM((4, 2, 4, 512, 128), BF),
            pltpu.VMEM((2, 128, ROWS), BF),
            pltpu.VMEM((2, 2, 128, ROWS), BF),
            pltpu.VMEM((2, 8, 128), F32),
            pltpu.VMEM((16, 256), BF),
            pltpu.VMEM((2, 2, 128, ROWS), F32),
            pltpu.VMEM((2, 2, 1, ROWS), F32),
            pltpu.VMEM((2, 2, 1, ROWS), F32),
            pltpu.VMEM((ROWS, ROWS), F32),
            pltpu.VMEM((ROWS, ROWS), F32),
            pltpu.VMEM((2, 1, ROWS), F32),
            pltpu.VMEM((512, 128), BF),
            pltpu.VMEM((2, ROWS, 128), BF),
            pltpu.VMEM((2, ROWS, 128), BF),
            pltpu.VMEM((ROWS, 256), BF),
            pltpu.VMEM((512, WIDE), BF),
            pltpu.VMEM((4, 8, 64, 1024), BF),
            pltpu.VMEM((4, 4, 64, 1024), BF),
            pltpu.VMEM((3, 4, 64, 1024), BF),
            pltpu.VMEM((4, 64, 1024), BF),
            pltpu.VMEM((2, 4, 64, 1024), BF),
            dma((4,)), dma((6,)), dma, dma, dma((2, 2)), dma((4, 2, 4)), dma((2,)), dma((2,)), dma((2,)), dma((2,)),
            dma, dma, dma((2, 4)), dma((2, 4)), dma((4, 4)), dma((2,)), dma((2,)),
            dma((4, 4)), dma((4, 4)), dma((3, 4)), dma((3, 4)),
        ],
        compiler_params=pltpu.CompilerParams(vmem_limit_bytes=67043328, collective_id=0, has_side_effects=True),
        name="mixer",
    )(tokens, norm_gain.reshape(1, WIDE), w_key, w_value, w_query, w_pool_in, lam, pool_mix.reshape(256, 64),
      pool_scale.reshape(1, 256), head_gain.reshape(1, 128), pool_proj, attn_proj)


def solution(mesh):
    return jax.shard_map(
        body,
        mesh=mesh,
        in_specs=(P("sp", None), P(), P(None, "tp"), P(None, "tp"), P(None, "tp"), P(None, "tp"),
                  P("tp", None, None), P("tp"), P("tp"), P(), P("tp", None), P("tp", None)),
        out_specs=P(("sp", "tp"), None),
        check_vma=False,
    )
```

```python
import jax
import jax.numpy as jnp
from jax import lax
from jax.experimental import pallas as pl
from jax.experimental.pallas import tpu as pltpu
from jax.sharding import PartitionSpec as P

EPS = 1e-6
NEG = -1e30
LOG2E = 1.4426950408889634
ROWS = 512
WIDE = 4096
SEG = 64
BF = jnp.bfloat16
F32 = jnp.float32
MESH_ID = pl.DeviceIdType.MESH
OUTER = ((2, 3, 0, 1), (0, 3, 1, 2), (3, 2, 1, 0), (1, 0, 3, 2))
INNER = ((0, 2, 1, 3), (2, 1, 3, 0), (1, 0, 3, 2), (3, 2, 1, 0))


def pick(at, values):
    packed = sum(value << (2 * i) for i, value in enumerate(values))
    packed = packed - (1 << 32) if packed >= 1 << 31 else packed
    return lax.shift_right_logical(jnp.int32(packed), 2 * at) & 3


def flat(table):
    return [value for row in table for value in row]


def inverse(table):
    return [row.index(value) for row in table for value in range(4)]
ANY = pl.BlockSpec(memory_space=pl.ANY)


def mixer_kernel(tok, gain_in, w_k, w_v, w_q, w_p, lam_hbm, mix_in, scale_in, head_gain_in, pool_proj, attn_proj,
                 out,
                 gain, lam, pool_mix, pool_scale, head_gain, out_buf, small_sem, out_sem, raw, normed, wts, kv_in, q_in, pool_in, lam_in, kv, qraw, qcat, lamb, rim, acc, top, den, sbank_a, sbank_b, smax, x_relay, ao, ab, pooled, w_out, pbuf, dbuf, sbuf, relay, fin,
                 tok_sem, w_sem, x_recv, pass_send, a2a_send, kv_recv, q_send, q_recv, lam_send, lam_recv, rim_send, rim_recv,
                 zp_send, zm_send, dd_send, ret_send, ret_recv, pd_send, pd_recv, y_send, y_recv):
    sbank = (sbank_a, sbank_b)
    sp = lax.axis_index("sp")
    tp = lax.axis_index("tp")
    z, x = lax.shift_right_logical(sp, 2), sp & 3
    y, c = lax.shift_right_logical(tp, 1), tp & 1

    def wrap(i):
        return (i + 4) & 3

    def dev(zz, xx, cc):
        return (zz * 4 + xx, y * 2 + cc)

    def at(off):
        return (x + off) & 3

    me = (sp, tp)

    def is_me(d):
        return (d[0] == sp) & (d[1] == tp)

    core_src = lax.div(x, 2)
    outer_row = (z == 0) | (z == 3)
    place = jnp.where(z < 2, x, 3 - x)
    cq = jnp.where(outer_row, 0, 1)
    sq = lax.div(z, 2)
    a_here, b_here = pick(x * 4 + z, flat(OUTER)), pick(x * 4 + z, flat(INNER))
    qb = [jnp.where(c == 0, a_here, 4 + b_here), jnp.where(c == 0, 15 - a_here, 11 - b_here)]
    partner = dev(z, x, 1 - c)
    z_up, z_dn = dev(wrap(z + 1), x, c), dev(wrap(z - 1), x, c)
    y_up = (sp, wrap(y + 1) * 2 + c)
    y_dn = (sp, wrap(y - 1) * 2 + c)
    nxt = (lax.rem(sp + 1, 16), tp)
    prv = (lax.rem(sp + 15, 16), tp)
    a2a_dst = [[dev(z, 2 * c + hh, hf) for hf in range(2)] for hh in range(2)]
    q_dst = []
    for hh in range(2):
        spot = (2 * c + hh) * 4 + place
        q_dst.append(dev(jnp.where(outer_row, pick(spot, inverse(OUTER)), pick(spot, inverse(INNER))), 2 * c + hh, cq))
    q_src = [dev(lax.div(qb[s], 4), lax.rem(qb[s], 4), core_src) for s in range(2)]

    def load(src, dst, sem):
        cp = pltpu.make_async_copy(src, dst, sem)
        cp.start()
        return cp

    tok_loads = [load(tok.at[pl.ds(r * 128, 128)], raw.at[pl.ds(r * 128, 128)], tok_sem.at[r]) for r in range(4)]
    small = [load(src, dst, small_sem.at[i]) for i, (src, dst) in enumerate(
        ((gain_in, gain), (lam_hbm, lam), (mix_in, pool_mix), (scale_in, pool_scale), (head_gain_in, head_gain)))]
    in_loads = []

    barrier = pltpu.get_barrier_semaphore()

    def greet(d):
        pl.semaphore_signal(barrier, inc=1, device_id=d, device_id_type=MESH_ID)

    behind, beyond = jnp.where(c == 0, at(3), at(1)), jnp.where(c == 0, at(1), at(3))
    greeted = [dev(z, at(off), core_src) for off in (0, 1, 3)] + [dev(z, behind, lax.div(beyond, 2)), dev(z, behind, c)]
    greeted = greeted + q_src + q_dst + [z_up, z_dn, partner, y_up, y_dn, prv]
    for d in greeted:
        greet(d)

    def remote(src, dst, ssem, rsem, d):
        return pltpu.make_async_remote_copy(src_ref=src, dst_ref=dst, send_sem=ssem, recv_sem=rsem,
                                            device_id=d, device_id_type=MESH_ID)

    def send_any(src, dst, ssem, rsem, d):
        @pl.when(is_me(d))
        def _():
            pltpu.make_async_copy(src, dst, rsem).start()

        @pl.when(jnp.logical_not(is_me(d)))
        def _():
            remote(src, dst, ssem, rsem, d).start()

    def sent_any(src, dst, ssem, rsem, d):
        @pl.when(jnp.logical_not(is_me(d)))
        def _():
            remote(src, dst, ssem, rsem, d).wait_send()

    def arrived(dst, rsem):
        pltpu.make_async_copy(dst, dst, rsem).wait()

    small[0].wait()
    with jax.named_scope("norm"):
        for r in range(4):
            tok_loads[r].wait()
            in_loads.append(load((w_q, w_k, w_v, w_p)[r], wts.at[r], w_sem.at[r]))

            @pl.loop(0, 8, unroll=4)
            def _(i):
                rows = pl.ds(pl.multiple_of(r * 128 + i * 16, 16), 16)
                wide = raw[rows].astype(F32)
                scale = lax.rsqrt(jnp.mean(wide * wide, axis=-1, keepdims=True) + EPS)
                normed[rows] = (wide * scale * gain[...]).astype(BF)

    def halves(i, finish_half):
        for r in range(2):
            rows = slice(256 * r, 256 * r + 256)
            finish_half(rows, jnp.dot(normed[rows], wts[i], preferred_element_type=F32))

    for cp in small[1:]:
        cp.wait()
    for hh in range(2):
        lam_in[hh] = jnp.full((8, 128), lam[hh], F32)
    with jax.named_scope("query"):
        in_loads[0].wait()

        def query_half(rows, value):
            value = value * (0.125 * LOG2E)
            for hh in range(2):
                q_in[hh, :, rows] = value[:, 128 * hh:128 * hh + 128].T.astype(BF)

        halves(0, query_half)
    pl.semaphore_wait(barrier, len(greeted))
    q_args = []
    for hh in range(2):
        q_args.append((q_in.at[hh], qraw.at[sq], q_send.at[hh], q_recv.at[sq], q_dst[hh]))
        q_args.append((lam_in.at[hh], lamb.at[sq], lam_send.at[hh], lam_recv.at[sq], q_dst[hh]))
    for a in q_args:
        send_any(*a)

    a2a_args = []
    for hh in range(2):
        for hf in range(2):
            a2a_args.append((kv_in.at[hh, hf], kv.at[z, hf, x], a2a_send.at[hh, hf], kv_recv.at[0, hf, x],
                             a2a_dst[hh][hf]))

    def hop_args(hh, hf):
        return (kv_in.at[hh, hf], x_relay, a2a_send.at[hh, hf], x_recv, dev(z, at(1 if hf == 0 else 3), hf))

    def exchange(hf):
        for hh in range(2):
            @pl.when(wrap(2 * c + hh - x) != 2)
            def _():
                send_any(*a2a_args[2 * hh + hf])

    def exchange_far(hf):
        for hh in range(2):
            @pl.when(wrap(2 * c + hh - x) == 2)
            def _():
                remote(*hop_args(hh, hf)).start()

    for i in range(1, 3):
        in_loads[i].wait()
    for hf in range(2):
        with jax.named_scope("keys_values"):
            rows = slice(256 * hf, 256 * hf + 256)
            keys = jnp.dot(normed[rows], wts[1], preferred_element_type=F32).astype(BF)
            values = jnp.dot(normed[rows], wts[2], preferred_element_type=F32)
            for hh in range(2):
                kv_in[hh, hf, 0:256] = keys[:, 128 * hh:128 * hh + 128]
                for j in range(2):
                    tile = values[128 * j:128 * j + 128, 128 * hh:128 * hh + 128]
                    kv_in[hh, hf, 256 + 128 * j:384 + 128 * j] = tile.T.astype(BF)
        exchange(hf)
    w_loads = [load(pool_proj, w_out.at[pl.ds(0, 256)], w_sem.at[4]),
               load(attn_proj, w_out.at[pl.ds(256, 256)], w_sem.at[5])]

    hop_from = jnp.where(c == 0, at(3), at(1))
    pass_args = (x_relay, kv.at[z, c, hop_from], pass_send, kv_recv.at[0, c, hop_from],
                 dev(z, jnp.where(c == 0, at(1), at(3)), c))


    def dd_args(rel, xk):
        piece = kv.at[wrap(z + rel), c, xk]
        return (piece, piece, dd_send.at[rel, xk], kv_recv.at[rel, c, xk], partner)

    def up_args(rel, xk):
        piece = kv.at[wrap(z + rel), c, xk]
        return (piece, piece, zp_send.at[rel & 1, xk], kv_recv.at[(rel + 3) % 4, c, xk], z_up)

    def dn_args(rel, xk):
        piece = kv.at[wrap(z + rel), c, xk]
        return (piece, piece, zm_send.at[rel & 1, xk], kv_recv.at[(rel + 1) % 4, c, xk], z_dn)

    def mine(rel, xk):
        arrived(kv.at[wrap(z + rel), c, xk], kv_recv.at[rel, c, xk])

    def go(args):
        remote(*args).start()

    mine(0, at(0))
    go(up_args(0, at(0)))
    go(dn_args(0, at(0)))
    go(dd_args(0, at(0)))

    with jax.named_scope("pool_in"):
        in_loads[3].wait()

        def pool_half(rows, value):
            pool_in[rows] = value.astype(BF)

        halves(3, pool_half)
    rim_args = (pool_in.at[pl.ds(ROWS - 16, 16)], rim, rim_send, rim_recv, nxt)
    remote(*rim_args).start()
    for hf in range(2):
        exchange_far(hf)

    with jax.named_scope("own_near"):
        mine(0, at(1))
        go(up_args(0, at(1)))
        go(dd_args(0, at(1)))
        mine(0, at(3))
        go(dn_args(0, at(3)))
        go(up_args(0, at(3)))
        go(dd_args(0, at(3)))
        arrived(x_relay, x_recv)
        go(pass_args)

    with jax.named_scope("queries"):
        for s in range(2):
            arrived(qraw.at[s], q_recv.at[s])
            arrived(lamb.at[s], lam_recv.at[s])
            q = qraw[s]
            zero = jnp.zeros((64, ROWS), BF)
            qcat[s, 0] = jnp.concatenate([q[:64], zero], axis=0)
            qcat[s, 1] = jnp.concatenate([zero, q[64:]], axis=0)
            for m in range(2):
                top[s, m] = jnp.full((1, ROWS), NEG, F32)
                den[s, m] = jnp.zeros((1, ROWS), F32)
                acc[s, m] = jnp.zeros((128, ROWS), F32)

    def score(bank, zk, xk, s, m):
        keys = jnp.concatenate([kv[zk, hf, xk, 0:256] for hf in range(2)], axis=0)
        scores = jnp.dot(keys, qcat[s, m], preferred_element_type=F32)
        sbank[bank][...] = scores
        smax[bank] = jnp.max(scores, axis=0, keepdims=True)

    def weigh(bank, zk, xk, s, m, masked):
        vals = jnp.concatenate([kv[zk, hf, xk, 256 + 128 * j:384 + 128 * j] for hf in range(2) for j in range(2)],
                               axis=1)
        scores = sbank[bank][...]
        peak = smax[bank]
        if masked:
            allowed = (lax.div(lax.broadcasted_iota(jnp.int32, (ROWS, ROWS), 0), SEG)
                       <= lax.div(lax.broadcasted_iota(jnp.int32, (ROWS, ROWS), 1), SEG))
            scores = jnp.where(allowed, scores, NEG)
            peak = jnp.max(scores, axis=0, keepdims=True)
        old = top[s, m]
        new = jnp.maximum(old, peak)
        probs = jnp.exp2(scores - new)
        shrink = jnp.exp2(old - new)
        top[s, m] = new
        den[s, m] = den[s, m] * shrink + jnp.sum(probs, axis=0, keepdims=True)
        acc[s, m] = acc[s, m] * shrink + jnp.dot(vals, probs.astype(BF), preferred_element_type=F32)

    def attend(here, ahead, slots, masked):
        tiles = [(s, m) for s in slots for m in range(2)]
        for n, (s, m) in enumerate(tiles):
            if n + 1 < len(tiles):
                score((n + 1) % 2, *here, *tiles[n + 1])
            else:
                score(0, *ahead, 1, 0)
            weigh(n % 2, *here, s, m, masked == s)

    def joined(rel, xk):
        arrived(kv.at[wrap(z + rel), 1 - c, xk], kv_recv.at[rel, 1 - c, xk])

    def visit(here, ahead):
        block = here[0] * 4 + here[1]

        @pl.when(block <= qb[1])
        def _():
            @pl.when(block > qb[0])
            def _():
                @pl.when(block < qb[1])
                def _():
                    attend(here, ahead, (1,), None)

                @pl.when(block == qb[1])
                def _():
                    attend(here, ahead, (1,), 1)

            @pl.when(block <= qb[0])
            def _():
                @pl.when(block < qb[0])
                def _():
                    attend(here, ahead, (1, 0), None)

                @pl.when(block == qb[0])
                def _():
                    attend(here, ahead, (1, 0), 0)

        @pl.when(block > qb[1])
        def _():
            score(0, *ahead, 1, 0)

    below, above = (0, 1, 3, 2), (0, 3, 2, 1)
    plan = [(0, 0), (0, 1), (0, 3), (3, 0), (1, 0), (0, 2), (3, 1), (1, 3), (3, 3), (1, 2), (3, 2), (1, 1),
            (2, 0), (2, 3), (2, 1), (2, 2)]

    def near(i):
        mine(3, at(below[i]))
        if i < 2:
            go(up_args(3, at(below[i])))
        go(dd_args(3, at(below[i])))
        mine(1, at(above[i]))
        if i in (1, 2):
            go(dn_args(1, at(above[i])))
        go(dd_args(1, at(above[i])))

    def far(i):
        for off in ((0, 3), (1, 2))[i]:
            mine(2, at(off))
            go(dd_args(2, at(off)))

    def pooling(_):
        arrived(rim, rim_recv)
        edge = jnp.where(sp == 0, 0.0, rim[...].astype(F32))
        own = pool_in[...].astype(F32)
        lane = lax.broadcasted_iota(jnp.int32, (1, 128), 1)
        totals = []
        for side in range(2):
            cols = slice(128 * side, 128 * side + 128)
            line = jnp.concatenate([edge[:, cols], own[:, cols]], axis=0)
            s2 = line + pltpu.roll(line, 1, 0)
            s4 = s2 + pltpu.roll(s2, 2, 0)
            if side == 0:
                totals.append(jnp.where(lane < 64, s2, s4)[16:])
            else:
                s8 = s4 + pltpu.roll(s4, 4, 0)
                s16 = s8 + pltpu.roll(s8, 8, 0)
                totals.append(jnp.where(lane < 64, s8, s16)[16:])
        total = jnp.concatenate(totals, axis=1)
        lane = lax.broadcasted_iota(jnp.int32, (1, 256), 1)
        window = jnp.where(lane < 64, 2, jnp.where(lane < 128, 4, jnp.where(lane < 192, 8, 16)))
        position = sp * ROWS + lax.broadcasted_iota(jnp.int32, (16, 256), 0)
        early = total[:16] / jnp.minimum(position + 1, window).astype(F32)
        later = total[16:] * (1.0 / window.astype(F32))
        mixed_in = (jnp.concatenate([early, later], axis=0) - own).astype(BF)
        spread = (lax.rem(lax.broadcasted_iota(jnp.int32, (64, 256), 1), 64)
                  == lax.broadcasted_iota(jnp.int32, (64, 256), 0)).astype(F32).astype(BF)
        wide_mix = jnp.dot(pool_mix[...], spread, preferred_element_type=F32)
        same = (lax.div(lax.broadcasted_iota(jnp.int32, (256, 256), 0), 64)
                == lax.div(lax.broadcasted_iota(jnp.int32, (256, 256), 1), 64))
        block_mix = jnp.where(same, wide_mix, 0.0).astype(BF)
        grouped = jnp.dot(mixed_in, block_mix, preferred_element_type=F32)
        pooled[...] = (grouped * pool_scale[...]).astype(BF)

    def own_far(_):
        mine(0, at(2))
        go(dn_args(0, at(2)))
        go(up_args(0, at(2)))
        go(dd_args(0, at(2)))
        go(dn_args(0, at(1)))

    service = {1: (near, 0), 3: (own_far, 0), 5: (near, 1), 7: (near, 2), 8: (near, 3), 9: (pooling, 0), 10: (far, 0),
               12: (far, 1)}

    mine_h = lax.rem(x, 2)
    ret_args = [(ao.at[s], ab.at[mine_h], ret_send.at[s], ret_recv.at[mine_h], q_src[s]) for s in range(2)]

    def finish(s):
        o1 = acc[s, 0] / den[s, 0]
        o2 = acc[s, 1] / den[s, 1]
        blend = o1 - lamb[s][0:1, 0:1] * o2
        scaled = blend * lax.rsqrt(jnp.mean(blend * blend, axis=0, keepdims=True) + EPS)
        ao[s] = (scaled.T * head_gain[...] * 0.8).astype(BF)
        send_any(*ret_args[s])

    soon = wrap(z + 2) * 4 > qb[0]

    with jax.named_scope("attend"):
        joined(0, at(0))
        score(0, z, at(0), 1, 0)

        @pl.loop(0, 16)
        def _(v):
            @pl.when(pick(v, [int(i in service) for i in range(16)]) == 1)
            def _():
                for when, (serve, i) in service.items():
                    @pl.when(v == when)
                    def _():
                        with jax.named_scope(f"serve{when}"):
                            serve(i)

            @pl.when((v == 12) & soon)
            def _():
                finish(0)

            follow = jnp.minimum(v + 1, 15)
            rel, nrel = (pick(i, [p[0] for p in plan]) for i in (v, follow))
            xk, nxk = (at(pick(i, [p[1] for p in plan])) for i in (v, follow))

            @pl.when(v < 15)
            def _():
                with jax.named_scope("join"):
                    joined(nrel, nxk)

            with jax.named_scope("visit"):
                visit((wrap(z + rel), xk), (wrap(z + nrel), nxk))

    with jax.named_scope("finish"):
        finish(1)

        @pl.when(jnp.logical_not(soon))
        def _():
            finish(0)

    with jax.named_scope("drain"):
        remote(*rim_args).wait_send()
        for a in a2a_args + q_args:
            sent_any(*a)
        remote(*pass_args).wait_send()
        for off in range(4):
            remote(*up_args(0, at(off))).wait_send()
            remote(*dn_args(0, at(off))).wait_send()
            for rel in range(4):
                remote(*dd_args(rel, at(off))).wait_send()
        for i in range(2):
            remote(*up_args(3, at(below[i]))).wait_send()
            remote(*dn_args(1, at(above[i + 1]))).wait_send()

    for cp in w_loads:
        cp.wait()
    with jax.named_scope("home"):
        for hh in range(2):
            arrived(ab.at[hh], ret_recv.at[hh])

    order = [wrap(y + 2), wrap(y + 1), wrap(y - 1), y]

    def pd_args(h, k):
        return (pbuf.at[h, 2 * order[k] + 1 - c], dbuf.at[h, k], pd_send.at[h, k], pd_recv.at[h, k], partner)

    def project(h):
        feats = jnp.concatenate([pooled[...], ab[0], ab[1]], axis=1)
        term = jnp.dot(feats, w_out[:, 512 * h:512 * h + 512], preferred_element_type=F32)
        pbuf[h] = term.astype(BF).reshape(8, 64, 512)
        for k in range(4):
            go(pd_args(h, k))

    def chip_sum(h, k):
        arrived(dbuf.at[h, k], pd_recv.at[h, k])
        return pbuf[h, 2 * order[k] + c].astype(F32) + dbuf[h, k].astype(F32)

    def relay_args(h):
        return (sbuf.at[0, h], relay.at[h], y_send.at[0, h], y_recv.at[0, h], y_up if h < 4 else y_dn)

    def up_sum_args(h):
        return (sbuf.at[1, h], fin.at[0, h], y_send.at[1, h], y_recv.at[1, h], y_up)

    def dn_sum_args(h):
        return (sbuf.at[2, h], fin.at[1, h], y_send.at[2, h], y_recv.at[2, h], y_dn)

    def put(i, h, value, args):
        sbuf[i, h] = value.astype(BF)
        go(args)

    def start_relay(h):
        put(0, h, chip_sum(h, 0), relay_args(h))

    def direct(h):
        if h < 4:
            put(2, h, chip_sum(h, 2), dn_sum_args(h))
        else:
            put(1, h, chip_sum(h, 1), up_sum_args(h))

    def relayed(h):
        own_sum = chip_sum(h, 1 if h < 4 else 2)
        arrived(relay.at[h], y_recv.at[0, h])
        value = own_sum + relay[h].astype(F32)
        if h < 4:
            put(1, h, value, up_sum_args(h))
        else:
            put(2, h, value, dn_sum_args(h))

    with jax.named_scope("out_first"):
        for h in range(4):
            project(h)
            project(h + 4)
            start_relay(h)
            start_relay(h + 4)
            direct(h)
            direct(h + 4)
    with jax.named_scope("out_relayed"):
        for h in range(4):
            relayed(h)
            relayed(h + 4)
    stores = []
    with jax.named_scope("out_last"):
        for h in (4, 0, 5, 1, 6, 2, 7, 3):
            own_sum = chip_sum(h, 3)
            arrived(fin.at[0, h], y_recv.at[1, h])
            arrived(fin.at[1, h], y_recv.at[2, h])
            whole = own_sum + fin[0, h].astype(F32) + fin[1, h].astype(F32)
            cols = pl.ds(512 * h, 512)
            out_buf[:, cols] = whole.astype(BF)
            stores.append(load(out_buf.at[:, cols], out.at[:, cols], out_sem.at[h]))

    for a in ret_args:
        sent_any(*a)
    for cp in stores:
        cp.wait()
    for h in range(8):
        for k in range(4):
            remote(*pd_args(h, k)).wait_send()
        remote(*relay_args(h)).wait_send()
        remote(*up_sum_args(h)).wait_send()
        remote(*dn_sum_args(h)).wait_send()


def body(tokens, norm_gain, w_pool_in, w_query, w_key, w_value, pool_mix, pool_scale, lam, head_gain,
         pool_proj, attn_proj):
    sd = jax.ShapeDtypeStruct
    dma = pltpu.SemaphoreType.DMA
    return pl.pallas_call(
        mixer_kernel,
        out_shape=sd((64, WIDE), BF),
        in_specs=[ANY] * 12,
        out_specs=ANY,
        scratch_shapes=[
            pltpu.VMEM((1, WIDE), F32),
            pltpu.SMEM((2,), F32),
            pltpu.VMEM((256, 64), BF),
            pltpu.VMEM((1, 256), F32),
            pltpu.VMEM((1, 128), F32),
            pltpu.VMEM((64, WIDE), BF),
            dma((5,)), dma((8,)),
            pltpu.VMEM((ROWS, WIDE), BF),
            pltpu.VMEM((ROWS, WIDE), BF),
            pltpu.VMEM((4, WIDE, 256), BF),
            pltpu.VMEM((2, 2, 512, 128), BF),
            pltpu.VMEM((2, 128, ROWS), BF),
            pltpu.VMEM((ROWS, 256), BF),
            pltpu.VMEM((2, 8, 128), F32),
            pltpu.VMEM((4, 2, 4, 512, 128), BF),
            pltpu.VMEM((2, 128, ROWS), BF),
            pltpu.VMEM((2, 2, 128, ROWS), BF),
            pltpu.VMEM((2, 8, 128), F32),
            pltpu.VMEM((16, 256), BF),
            pltpu.VMEM((2, 2, 128, ROWS), F32),
            pltpu.VMEM((2, 2, 1, ROWS), F32),
            pltpu.VMEM((2, 2, 1, ROWS), F32),
            pltpu.VMEM((ROWS, ROWS), F32),
            pltpu.VMEM((ROWS, ROWS), F32),
            pltpu.VMEM((2, 1, ROWS), F32),
            pltpu.VMEM((512, 128), BF),
            pltpu.VMEM((2, ROWS, 128), BF),
            pltpu.VMEM((2, ROWS, 128), BF),
            pltpu.VMEM((ROWS, 256), BF),
            pltpu.VMEM((512, WIDE), BF),
            pltpu.VMEM((8, 8, 64, 512), BF),
            pltpu.VMEM((8, 4, 64, 512), BF),
            pltpu.VMEM((3, 8, 64, 512), BF),
            pltpu.VMEM((8, 64, 512), BF),
            pltpu.VMEM((2, 8, 64, 512), BF),
            dma((4,)), dma((6,)), dma, dma, dma((2, 2)), dma((4, 2, 4)), dma((2,)), dma((2,)), dma((2,)), dma((2,)),
            dma, dma, dma((2, 4)), dma((2, 4)), dma((4, 4)), dma((2,)), dma((2,)),
            dma((8, 4)), dma((8, 4)), dma((3, 8)), dma((3, 8)),
        ],
        compiler_params=pltpu.CompilerParams(vmem_limit_bytes=67043328, collective_id=0, has_side_effects=True),
        name="mixer",
    )(tokens, norm_gain.reshape(1, WIDE), w_key, w_value, w_query, w_pool_in, lam, pool_mix.reshape(256, 64),
      pool_scale.reshape(1, 256), head_gain.reshape(1, 128), pool_proj, attn_proj)


def solution(mesh):
    return jax.shard_map(
        body,
        mesh=mesh,
        in_specs=(P("sp", None), P(), P(None, "tp"), P(None, "tp"), P(None, "tp"), P(None, "tp"),
                  P("tp", None, None), P("tp"), P("tp"), P(), P("tp", None), P("tp", None)),
        out_specs=P(("sp", "tp"), None),
        check_vma=False,
    )
```
